32 devices in a mesh: rep: 2 (over x), fs: 8 (over z, y), tp: 2 (over core).
Axes of the slice: x: 2, y: 2, z: 4, core: 2. Of those that a mesh axis runs over, the one named last changes fastest.
Arguments:
- tokens: bfloat16 [5120, 2048], P(('rep', 'fs')), may hold values from -6 to 6
- mixer_out: bfloat16 [5120, 2048], P(('rep', 'fs')), may hold values from -6 to 6
- gate_first: bfloat16 [2048, 2816], P('fs', 'tp'), may hold values from -0.125 to 0.125
- up_first: bfloat16 [2048, 2816], P('fs', 'tp'), may hold values from -0.125 to 0.125
- down_first: bfloat16 [2816, 2048], P('tp', 'fs'), may hold values from -0.3125 to 0.3125
- gate_second: bfloat16 [2048, 2816], P('fs', 'tp'), may hold values from -0.125 to 0.125
- up_second: bfloat16 [2048, 2816], P('fs', 'tp'), may hold values from -0.125 to 0.125
- down_second: bfloat16 [2816, 2048], P('tp', 'fs'), may hold values from -0.3125 to 0.3125
- gain_first: float32 [2048], replicated, may hold values from 0.1 to 1.9
- bias_first: float32 [2048], replicated, may hold values from -1.5 to 1.5
- gain_middle: float32 [2048], replicated, may hold values from 0.1 to 1.9
- bias_middle: float32 [2048], replicated, may hold values from -1.5 to 1.5
- gain_last: float32 [2048], replicated, may hold values from 0.1 to 1.9
- bias_last: float32 [2048], replicated, may hold values from -1.5 to 1.5
Outputs:
- layer_out: bfloat16 [5120, 2048], P(('rep', 'fs'))
The draws below stay inside these ranges and needn't reach their ends.
All inputs are finite; a program needn't handle non-finite values.
Results may differ from the reference program's by a relative error of at most 0.014.
Values may be sent and summed in bfloat16 or wider, within the bound.
A program may use at most 64 MiB of HBM per device.

```python
import math
import jax
import jax.numpy as jnp
from jax import lax

D = 2048
FF = 2816
TOKENS = 5120
N_TP = 2


def level_of(own_key, extent, shards, low, high):
    loudness, own = 1.0, jax.random.fold_in(own_key, 6)
    for axis_at, parts in shards:
        draws = jnp.exp(jax.random.uniform(jax.random.fold_in(own, axis_at), (parts,), jnp.float32, low / len(shards), high / len(shards)))
        loudness = loudness * jnp.repeat(draws, extent[axis_at] // parts).reshape([-1 if axis == axis_at else 1 for axis in range(len(extent))])
    return loudness


def normal_values(own_key, shape, width, bound, cuts=(), kind=jnp.bfloat16):
    result = width * jax.random.normal(own_key, shape, jnp.float32)
    if cuts:
        result = result * level_of(own_key, shape, cuts, -0.22, 0.18)
    return jnp.clip(result, -bound, bound).astype(kind)


def setup_inputs(seed: int = 0) -> dict:
    seeds = jax.random.split(jax.random.key(seed), 15)
    tokens = normal_values(seeds[0], (TOKENS, D), 1.0, 6.0, ((0, 16),))
    mixer_out = normal_values(seeds[1], (TOKENS, D), 1.0, 6.0, ((0, 16),))
    gate_first = normal_values(seeds[2], (D, FF), D ** -0.5, 0.125, ((0, 8), (1, 2)))
    up_first = normal_values(seeds[3], (D, FF), D ** -0.5, 0.125, ((0, 8), (1, 2)))
    down_first = normal_values(seeds[4], (FF, D), (FF // 8) ** -0.5, 0.3125, ((0, 2), (1, 8)))
    gate_second = normal_values(seeds[5], (D, FF), D ** -0.5, 0.125, ((0, 8), (1, 2)))
    up_second = normal_values(seeds[6], (D, FF), D ** -0.5, 0.125, ((0, 8), (1, 2)))
    down_second = normal_values(seeds[7], (FF, D), (FF // 8) ** -0.5, 0.3125, ((0, 2), (1, 8)))
    gain_first = jnp.clip(1.0 + 0.18 * jax.random.normal(seeds[8], (D,), jnp.float32), 0.1, 1.9)
    bias_first = normal_values(seeds[9], (D,), 0.3, 1.5, (), jnp.float32)
    gain_middle = jnp.clip(1.0 + 0.18 * jax.random.normal(seeds[10], (D,), jnp.float32), 0.1, 1.9)
    bias_middle = normal_values(seeds[11], (D,), 0.3, 1.5, (), jnp.float32)
    gain_last = jnp.clip(1.0 + 0.18 * jax.random.normal(seeds[12], (D,), jnp.float32), 0.1, 1.9)
    bias_last = normal_values(seeds[13], (D,), 0.3, 1.5, (), jnp.float32)
    return dict(tokens=tokens, mixer_out=mixer_out, gate_first=gate_first, up_first=up_first, down_first=down_first, gate_second=gate_second, up_second=up_second, down_second=down_second, gain_first=gain_first, bias_first=bias_first, gain_middle=gain_middle, bias_middle=bias_middle, gain_last=gain_last, bias_last=bias_last)


residual_scale = math.sqrt(2.0)
norm_eps = 1e-05

def normalize(summed, scaling, offset):
    center = summed - lax.optimization_barrier(jnp.mean(summed, axis=-1, keepdims=True))
    spread = lax.optimization_barrier(jnp.mean(center * center, axis=-1, keepdims=True))
    return center * lax.rsqrt(spread + norm_eps) * scaling.astype(jnp.float32) + offset.astype(jnp.float32)

def half_step(inputs, gate_weight, up_weight, down_weight):
    gate = jnp.dot(inputs, gate_weight, preferred_element_type=jnp.float32)
    value = jnp.dot(inputs, up_weight, preferred_element_type=jnp.float32)
    hidden = (jax.nn.silu(gate) * value).astype(jnp.bfloat16)
    block_size = hidden.shape[1] // N_TP
    running = jnp.zeros((inputs.shape[0], down_weight.shape[1]), jnp.float32)
    for member in range(N_TP):
        partial_value = jnp.dot(hidden[:, member * block_size:(member + 1) * block_size], down_weight[member * block_size:(member + 1) * block_size], preferred_element_type=jnp.float32)
        running = running + partial_value.astype(jnp.bfloat16).astype(jnp.float32)
    return running.astype(jnp.bfloat16)

def reference(tokens, mixer_out, gate_first, up_first, down_first, gate_second, up_second, down_second, gain_first, bias_first, gain_middle, bias_middle, gain_last, bias_last):
    first_branch = half_step(tokens, gate_first, up_first, down_first)
    first_norm = normalize(residual_scale * tokens.astype(jnp.float32) + 0.5 * first_branch.astype(jnp.float32), gain_first, bias_first).astype(jnp.bfloat16)
    middle_norm = normalize(residual_scale * first_norm.astype(jnp.float32) + mixer_out.astype(jnp.float32), gain_middle, bias_middle).astype(jnp.bfloat16)
    second_branch = half_step(middle_norm, gate_second, up_second, down_second)
    return normalize(residual_scale * middle_norm.astype(jnp.float32) + 0.5 * second_branch.astype(jnp.float32), gain_last, bias_last).astype(jnp.bfloat16)
```

```python
import math

import jax
import jax.numpy as jnp
from jax import lax
from jax.experimental import pallas as pl
from jax.experimental.pallas import tpu as pltpu
from jax.sharding import PartitionSpec as P

residual_scale = math.sqrt(2.0)
norm_eps = 1e-05
ZS, YS = 4, 2
F32, BF16 = jnp.float32, jnp.bfloat16


def normalize(summed, scaling, offset):
    center = summed - jnp.mean(summed, axis=-1, keepdims=True)
    spread = jnp.mean(center * center, axis=-1, keepdims=True)
    return center * lax.rsqrt(spread + norm_eps) * scaling + offset


def half_step(inputs, gate_weight, up_weight, down_weight):
    gate = jnp.dot(inputs, lax.all_gather(gate_weight, "fs", axis=0, tiled=True), preferred_element_type=F32)
    value = jnp.dot(inputs, lax.all_gather(up_weight, "fs", axis=0, tiled=True), preferred_element_type=F32)
    hidden = (jax.nn.silu(gate) * value).astype(BF16)
    partials = jnp.dot(hidden, lax.all_gather(down_weight, "fs", axis=1, tiled=True), preferred_element_type=F32)
    return lax.psum(partials.astype(BF16), "tp")


def per_device_general(
    tokens, mixer_out, gate_first, up_first, down_first, gate_second, up_second, down_second,
    gain_first, bias_first, gain_middle, bias_middle, gain_last, bias_last,
):
    first_branch = half_step(tokens, gate_first, up_first, down_first)
    first_norm = normalize(
        residual_scale * tokens.astype(F32) + 0.5 * first_branch.astype(F32), gain_first, bias_first
    ).astype(BF16)
    middle_norm = normalize(
        residual_scale * first_norm.astype(F32) + mixer_out.astype(F32), gain_middle, bias_middle
    ).astype(BF16)
    second_branch = half_step(middle_norm, gate_second, up_second, down_second)
    return normalize(
        residual_scale * middle_norm.astype(F32) + 0.5 * second_branch.astype(F32), gain_last, bias_last
    ).astype(BF16)


def slot_of(step):
    return step % ZS


STEPS = range(1, ZS)
WAYS = [(way, d, dy) for way in ("up", "dn") for d in STEPS for dy in range(YS)]
MAIN, EXTRA, DOWN = range(3)
GATE_UP = (MAIN, EXTRA)


def kernel(
    tokens_ref, mixer_ref, g1_ref, u1_ref, e1_ref, d1_ref, g2_ref, u2_ref, e2_ref, d2_ref,
    gain1_ref, bias1_ref, gain2_ref, bias2_ref, gain3_ref, bias3_ref,
    out_ref,
    gum, gux, dn, xb, acc, low, high, hid, keep, psend, precv, xsend, xrecv, ysend, yrecv, br, mix, fin,
    zs_send, zs_recv, ys_send, ys_recv, ag_send, ag_recv, rs_send, rs_recv, fin_send, fin_recv, local,
):
    rep, fs, core = lax.axis_index("rep"), lax.axis_index("fs"), lax.axis_index("tp")
    z, y = fs // YS, fs % YS
    quarter = fin.shape[0]
    half = 4 * quarter
    ks = gum.shape[2] // YS
    main = gum.shape[3] // 2
    fold = gux.shape[2] // YS
    extra = gux.shape[3] // 4
    wide = low.shape[1]
    dcols = dn.shape[3]
    own_q, pair_q = rep * YS + y, rep * YS + 1 - y

    pair = {"fs": z * YS + 1 - y}
    other_core = {"tp": 1 - core}
    near = {"rep": lax.rem(rep + core, 2), "fs": z * YS + lax.rem(y + 1 - core, YS)}
    far = {"rep": lax.rem(rep + 1 - core, 2), "fs": z * YS + lax.rem(y + core, YS)}

    def ds(first, count, unit):
        return pl.ds(pl.multiple_of(first, unit), count)

    mine, sib = ds(core * quarter, quarter, quarter), ds((1 - core) * quarter, quarter, quarter)
    weights = ((g1_ref, u1_ref, e1_ref, d1_ref), (g2_ref, u2_ref, e2_ref, d2_ref))

    def pieces(f, q):
        gate, up, ex, down = weights[f]
        rows, mrows, ex_rows = ds(y * ks, ks, ks), ds(q * main, main, main), ds(4 * main + q * extra, extra, 32)
        return (
            (gate.at[:, ds(q * main, main, main)], gum.at[f, 0, rows, pl.ds(0, main)]),
            (up.at[:, ds(q * main, main, main)], gum.at[f, 0, rows, pl.ds(main, main)]),
            (ex.at[q], gux.at[f, 0, ds(y * fold, fold, fold)]),
            (down.at[mrows], dn.at[f, y, pl.ds(0, main)]),
            (down.at[ex_rows], dn.at[f, y, pl.ds(main, extra)]),
        )

    loads = [
        [pltpu.make_async_copy(src, dst, local.at[5 * f + i]) for i, (src, dst) in enumerate(pieces(f, own_q))]
        for f in range(2)
    ]
    token_loads = [
        pltpu.make_async_copy(tokens_ref.at[mine], xb.at[0, pl.ds(0, quarter)], local.at[10]),
        pltpu.make_async_copy(tokens_ref.at[sib], xb.at[0, pl.ds(half, quarter)], local.at[11]),
    ]
    mixer_load = pltpu.make_async_copy(mixer_ref.at[mine], mix, local.at[12])
    for load in loads[0][:3] + token_loads + loads[0][3:] + loads[1] + [mixer_load]:
        load.start()

    barrier = pltpu.get_barrier_semaphore()

    def greet(target):
        pl.semaphore_signal(barrier, inc=1, device_id=target, device_id_type=pl.DeviceIdType.MESH)

    def plane(dz):
        return {"fs": lax.rem(z + dz + ZS, ZS) * YS + y}

    for target in (near, far, other_core):
        greet(target)

    @pl.when(z < ZS - 1)
    def _():
        greet(plane(1))

    @pl.when(z > 0)
    def _():
        greet(plane(-1))

    inner = jnp.logical_and(z > 0, z < ZS - 1)

    @pl.when(inner)
    def _():
        pl.semaphore_wait(barrier, 5)

    @pl.when(jnp.logical_not(inner))
    def _():
        pl.semaphore_wait(barrier, 4)

    sent = []

    def remote(src, dst, send_sem, recv_sem, target):
        return pltpu.make_async_remote_copy(
            src_ref=src, dst_ref=dst, send_sem=send_sem, recv_sem=recv_sem,
            device_id=target, device_id_type=pl.DeviceIdType.MESH,
        )

    def send(copy):
        copy.start()
        sent.append(copy)

    def pair_copy(f, i):
        src, dst = pieces(f, pair_q)[i]
        return remote(src, dst, ys_send.at[f, i], ys_recv.at[f, i], pair)

    def pair_landing(f, i):
        gate_rows = ds((1 - y) * ks, ks, ks)
        dst = (
            gum.at[f, 0, gate_rows, pl.ds(0, main)], gum.at[f, 0, gate_rows, pl.ds(main, main)],
            gux.at[f, 0, ds((1 - y) * fold, fold, fold)],
            dn.at[f, 1 - y, pl.ds(0, main)], dn.at[f, 1 - y, pl.ds(main, extra)],
        )[i]
        return remote(dst, dst, ys_send.at[f, i], ys_recv.at[f, i], pair)

    def pair_start(f, which):
        for i in which:
            send(pair_copy(f, i))

    def pair_wait(f, which):
        for i in which:
            pair_landing(f, i).wait_recv()

    def z_copy(f, piece, name):
        way, d, dy = name
        ya = lax.rem(y + dy, YS)
        sign = -1 if way == "up" else 1

        def at(n):
            if piece == MAIN:
                return gum.at[f, n, ds(ya * ks, ks, ks)]
            if piece == EXTRA:
                return gux.at[f, n, ds(ya * fold, fold, fold)]
            return dn.at[f, n * YS + ya]

        sems = zs_send.at[f, piece, WAYS.index(name)], zs_recv.at[f, piece, WAYS.index(name)]
        return remote(at(slot_of(sign * (d - 1))), at(slot_of(sign * d)), *sems, plane(-sign))

    def sends_up(d):
        return jnp.logical_and(z >= d - 1, z < ZS - 1)

    def sends_dn(d):
        return jnp.logical_and(z + d - 1 <= ZS - 1, z > 0)

    def gets_up(d):
        return z >= d

    def gets_dn(d):
        return z + d <= ZS - 1

    def own_send(f, which, dy):
        for way, does in (("up", sends_up), ("dn", sends_dn)):
            @pl.when(does(1))
            def _():
                for piece in which:
                    z_copy(f, piece, (way, 1, dy)).start()

    def relay(f, which, d, dys=range(YS)):
        for dy in dys:
            for way, gets, does in (("up", gets_up, sends_up), ("dn", gets_dn, sends_dn)):
                @pl.when(gets(d))
                def _():
                    for piece in which:
                        z_copy(f, piece, (way, d, dy)).wait_recv()
                        if d < ZS - 1:
                            @pl.when(does(d + 1))
                            def _():
                                z_copy(f, piece, (way, d + 1, dy)).start()

    def gather(f, i):
        target = (near, far, far)[i] if i < 3 else other_core
        src = (0, 0, 1)[i] if i < 3 else i - 3
        dst = i + 1 if i < 3 else i + 1
        return remote(
            xb.at[f, pl.ds(src * quarter, quarter)], xb.at[f, pl.ds(dst * quarter, quarter)],
            ag_send.at[f, i], ag_recv.at[f, i], target,
        )

    def gather_start(f):
        send(gather(f, 0))
        send(gather(f, 1))
        if f:
            send(gather(f, 3))

    def gather_near(f):
        gather(f, 0).wait_recv()
        send(gather(f, 2))
        send(gather(f, 4))

    def gather_far(f):
        gather(f, 1).wait_recv()
        send(gather(f, 5))
        gather(f, 2).wait_recv()
        send(gather(f, 6))

    def gather_wait(f):
        for i in range(3 if f else 4, 7):
            gather(f, i).wait_recv()

    step = 2 * quarter

    def gate_up(f, dz, first=False):
        n, zz = lax.rem(dz + ZS, ZS), z + dz
        base = zz * YS * ks

        @pl.loop(0, 4)
        def _(i):
            rows = ds(i * step, step, step)
            folded = [
                jnp.concatenate(
                    [xb[f, rows, ds(base + at * ks + h * fold, fold, fold)] for at in range(YS)], axis=1
                )
                for h in range(2)
            ]
            parts = (
                (acc, jnp.dot(xb[f, rows, ds(base, YS * ks, YS * ks)], gum[f, n], preferred_element_type=F32)),
                (low, jnp.dot(folded[0], gux[f, n, :, :wide], preferred_element_type=F32)),
                (high, jnp.dot(folded[1], gux[f, n, :, 4 * extra - wide:], preferred_element_type=F32)),
            )
            for total, part in parts:
                if first:
                    total[rows, :] = part
                else:
                    total[rows, :] += part

    def at_distance(d, act):
        if d == 0:
            act(0)
            return

        @pl.loop(0, 2)
        def _(i):
            dz = (2 * i - 1) * d

            @pl.when(jnp.logical_and(z + dz >= 0, z + dz < ZS))
            def _():
                act(dz)

    def both(d, act):
        def slots(dz):
            @pl.loop(0, YS)
            def _(ya):
                act(dz, ya)

        at_distance(d, slots)

    def gated(gate, value):
        return gate / (1.0 + jnp.exp(-gate)) * value

    def activate():
        shift = 2 * extra - (4 * extra - wide)
        some = -(-extra // 128) * 128

        @pl.loop(0, 8 * quarter // 32)
        def _(i):
            rows = ds(i * 32, 32, 32)
            hid[rows, :main] = gated(acc[rows, :main], acc[rows, main:]).astype(BF16)
            rest = low[rows, :] + pltpu.roll(high[rows, :], wide - shift, axis=1)
            value = pltpu.roll(rest, wide - extra, axis=1)
            made = gated(rest[:, :some], value[:, :some])
            hid[rows, main:] = made[:, :extra].astype(BF16)

    def index(dz, ya):
        return lax.rem(dz + ZS, ZS) * YS + ya

    def to_sibling(f, n):
        return remote(psend.at[f, n], precv.at[f, n], rs_send.at[f, 0, n], rs_recv.at[f, 0, n], other_core)

    def to_far(f, n):
        return remote(xsend.at[f, n], xrecv.at[f, n], rs_send.at[f, 1, n], rs_recv.at[f, 1, n], far)

    def to_near(f, n):
        return remote(ysend.at[f, n], yrecv.at[f, n], rs_send.at[f, 2, n], rs_recv.at[f, 2, n], near)

    def down_slot(f, dz, ya):
        n = index(dz, ya)
        psend[f, n] = jnp.dot(hid[half:, :], dn[f, n], preferred_element_type=F32).astype(BF16)
        to_sibling(f, n).start()
        keep[n] = jnp.dot(hid[:half, :], dn[f, n], preferred_element_type=F32)

    def add_cores(f, dz, ya):
        n = index(dz, ya)
        to_sibling(f, n).wait_recv()
        xsend[f, n] = (keep[n, 2 * quarter:, :] + precv[f, n, 2 * quarter:, :].astype(F32)).astype(BF16)
        to_far(f, n).start()
        keep[n, :2 * quarter, :] = keep[n, :2 * quarter, :] + precv[f, n, :2 * quarter, :].astype(F32)

    def add_far(f, dz, ya):
        n = index(dz, ya)
        to_far(f, n).wait_recv()
        ysend[f, n] = (keep[n, quarter:2 * quarter, :] + xrecv[f, n, quarter:, :].astype(F32)).astype(BF16)
        to_near(f, n).start()
        keep[n, :quarter, :] = keep[n, :quarter, :] + xrecv[f, n, :quarter, :].astype(F32)

    def add_near(f, dz, ya):
        n = index(dz, ya)
        to_near(f, n).wait_recv()
        cols = ds(((z + dz) * YS + ya) * dcols, dcols, dcols)
        br[:, cols] = keep[n, :quarter, :] + yrecv[f, n].astype(F32)

    def down(f, d):
        both(d, lambda dz, ya: down_slot(f, dz, ya))
        both(d, lambda dz, ya: add_cores(f, dz, ya))

    def first_norms():
        @pl.loop(0, quarter // 16)
        def _(i):
            rows = ds(i * 16, 16, 16)
            first = normalize(
                residual_scale * xb[0, rows, :].astype(F32) + 0.5 * br[rows, :], gain1_ref[...], bias1_ref[...]
            ).astype(BF16)
            xb[1, rows, :] = normalize(
                residual_scale * first.astype(F32) + mix[rows, :].astype(F32), gain2_ref[...], bias2_ref[...]
            ).astype(BF16)

    def last_norm():
        @pl.loop(0, quarter // 16)
        def _(i):
            rows = ds(i * 16, 16, 16)
            fin[rows, :] = normalize(
                residual_scale * xb[1, rows, :].astype(F32) + 0.5 * br[rows, :], gain3_ref[...], bias3_ref[...]
            ).astype(BF16)

    def load_wait(f, which):
        for i in which:
            loads[f][i].wait()

    pair_start(0, range(3))
    load_wait(0, range(3))
    own_send(0, GATE_UP, 0)
    token_loads[0].wait()
    gather_start(0)
    pair_start(0, (3, 4))
    load_wait(0, (3, 4))
    own_send(0, (DOWN,), 0)
    pair_wait(0, range(3))
    own_send(0, GATE_UP, 1)
    relay(0, GATE_UP, 1, (0,))
    gather_near(0)
    relay(0, GATE_UP, 1, (1,))
    gather_far(0)
    pair_start(1, range(3))
    token_loads[1].wait()
    gather_wait(0)
    gate_up(0, 0, first=True)
    relay(0, GATE_UP, 2, (0,))
    at_distance(1, lambda dz: gate_up(0, dz))
    relay(0, GATE_UP, 2, (1,))
    pair_wait(0, (3, 4))
    own_send(0, (DOWN,), 1)
    relay(0, (DOWN,), 1)
    pair_start(1, (3, 4))
    at_distance(2, lambda dz: gate_up(0, dz))
    relay(0, GATE_UP, 3)
    at_distance(3, lambda dz: gate_up(0, dz))
    relay(0, (DOWN,), 2)
    load_wait(1, range(5))
    own_send(1, GATE_UP, 0)
    pair_wait(1, range(3))
    own_send(1, GATE_UP, 1)
    for f in range(2):
        activate()
        down(f, 0)
        down(f, 1)
        both(0, lambda dz, ya: add_far(f, dz, ya))
        down(f, 2)
        both(1, lambda dz, ya: add_far(f, dz, ya))
        both(0, lambda dz, ya: add_near(f, dz, ya))
        relay(f, (DOWN,), 3)
        down(f, 3)
        both(2, lambda dz, ya: add_far(f, dz, ya))
        both(1, lambda dz, ya: add_near(f, dz, ya))
        both(3, lambda dz, ya: add_far(f, dz, ya))
        both(2, lambda dz, ya: add_near(f, dz, ya))
        both(3, lambda dz, ya: add_near(f, dz, ya))
        if f == 0:
            mixer_load.wait()
            first_norms()
            gather_start(1)
            relay(1, GATE_UP, 1)
            gather_near(1)
            relay(1, GATE_UP, 2)
            own_send(1, (DOWN,), 0)
            pair_wait(1, (3, 4))
            own_send(1, (DOWN,), 1)
            gather_far(1)
            gather_wait(1)
            gate_up(1, 0, first=True)
            at_distance(1, lambda dz: gate_up(1, dz))
            relay(1, (DOWN,), 1)
            at_distance(2, lambda dz: gate_up(1, dz))
            relay(1, (DOWN,), 2)
            relay(1, GATE_UP, 3)
            at_distance(3, lambda dz: gate_up(1, dz))
    last_norm()
    put = pltpu.make_async_copy(fin, out_ref.at[mine], local.at[13])
    put.start()
    over = remote(fin, out_ref.at[mine], fin_send.at[0], fin_recv.at[0], other_core)
    over.start()
    over.wait()
    put.wait()
    for copy in sent:
        copy.wait_send()
    for f in range(2):
        @pl.loop(0, ZS * YS)
        def _(n):
            for copy in (to_sibling(f, n), to_far(f, n), to_near(f, n)):
                copy.wait_send()

        for d in STEPS:
            for way, does in (("up", sends_up), ("dn", sends_dn)):
                @pl.when(does(d))
                def _():
                    for piece in range(3):
                        for dy in range(YS):
                            z_copy(f, piece, (way, d, dy)).wait_send()


def per_device(
    tokens, mixer_out, gate_first, up_first, down_first, gate_second, up_second, down_second,
    gain_first, bias_first, gain_middle, bias_middle, gain_last, bias_last,
):
    rows, width = tokens.shape
    ks, hidden = gate_first.shape
    dcols = down_first.shape[1]
    quarter = rows // 2
    main, extra = split(hidden)
    wide = -(-2 * extra // 128) * 128
    slots = ZS * YS

    def leftovers(gate, up):
        def part(w, h, q):
            return w[h * (ks // 2):(h + 1) * (ks // 2), 4 * main + q * extra:4 * main + (q + 1) * extra]

        return jnp.stack([
            jnp.concatenate([part(w, h, q) for h in range(2) for w in (gate, up)], axis=1) for q in range(4)
        ])

    any_spec, vmem = pl.BlockSpec(memory_space=pl.ANY), pl.BlockSpec(memory_space=pltpu.VMEM)
    vec = lambda v: v.reshape(1, width)
    dma = pltpu.SemaphoreType.DMA
    return pl.pallas_call(
        kernel,
        out_shape=jax.ShapeDtypeStruct((rows, width), BF16),
        in_specs=[any_spec] * 10 + [vmem] * 6,
        out_specs=any_spec,
        scratch_shapes=[
            pltpu.VMEM((2, ZS, YS * ks, 2 * main), BF16),
            pltpu.VMEM((2, ZS, YS * ks // 2, 4 * extra), BF16),
            pltpu.VMEM((2, slots, main + extra, dcols), BF16),
            pltpu.VMEM((2, 8 * quarter, width), BF16),
            pltpu.VMEM((8 * quarter, 2 * main), F32),
            pltpu.VMEM((8 * quarter, wide), F32),
            pltpu.VMEM((8 * quarter, wide), F32),
            pltpu.VMEM((8 * quarter, main + extra), BF16),
            pltpu.VMEM((slots, 4 * quarter, dcols), F32),
            pltpu.VMEM((2, slots, 4 * quarter, dcols), BF16),
            pltpu.VMEM((2, slots, 4 * quarter, dcols), BF16),
            pltpu.VMEM((2, slots, 2 * quarter, dcols), BF16),
            pltpu.VMEM((2, slots, 2 * quarter, dcols), BF16),
            pltpu.VMEM((2, slots, quarter, dcols), BF16),
            pltpu.VMEM((2, slots, quarter, dcols), BF16),
            pltpu.VMEM((quarter, width), F32),
            pltpu.VMEM((quarter, width), BF16),
            pltpu.VMEM((quarter, width), BF16),
            dma((2, 3, len(WAYS))), dma((2, 3, len(WAYS))),
            dma((2, 5)), dma((2, 5)),
            dma((2, 7)), dma((2, 7)),
            dma((2, 3, slots)), dma((2, 3, slots)),
            dma((1,)), dma((1,)),
            dma((14,)),
        ],
        compiler_params=pltpu.CompilerParams(
            collective_id=0, has_side_effects=True, vmem_limit_bytes=60 * 1024 * 1024
        ),
    )(
        tokens, mixer_out,
        gate_first, up_first, leftovers(gate_first, up_first), down_first,
        gate_second, up_second, leftovers(gate_second, up_second), down_second,
        vec(gain_first), vec(bias_first), vec(gain_middle), vec(bias_middle), vec(gain_last), vec(bias_last),
    )


def split(hidden):
    main = hidden // 4 // 128 * 128
    return main, hidden // 4 - main


def on_mesh(mesh, rows, width, hidden):
    sizes = dict(mesh.shape)
    if (sizes["rep"], sizes["fs"], sizes["tp"]) != (2, ZS * YS, 2):
        return False
    rows, ks, hidden = rows // (2 * ZS * YS), width // (ZS * YS), hidden // 2
    main, extra = split(hidden)
    return rows % 32 == 0 and ks % 256 == 0 and hidden % 128 == 0 and main > 0 and extra > 0 and extra % 32 == 0


def solution(mesh):
    def run(tokens, mixer_out, gate_first, *rest):
        fits = on_mesh(mesh, tokens.shape[0], tokens.shape[1], gate_first.shape[1])
        return jax.shard_map(
            per_device if fits else per_device_general,
            mesh=mesh,
            in_specs=(
                P(("rep", "fs"), None), P(("rep", "fs"), None),
                P("fs", "tp"), P("fs", "tp"), P("tp", "fs"),
                P("fs", "tp"), P("fs", "tp"), P("tp", "fs"),
                P(), P(), P(), P(), P(), P(),
            ),
            out_specs=P(("rep", "fs"), None),
            check_vma=False,
        )(tokens, mixer_out, gate_first, *rest)

    return run
```

```python
import math

import jax
import jax.numpy as jnp
from jax import lax
from jax.experimental import pallas as pl
from jax.experimental.pallas import tpu as pltpu
from jax.sharding import PartitionSpec as P

residual_scale = math.sqrt(2.0)
norm_eps = 1e-05
ZS, YS = 4, 2
F32, BF16 = jnp.float32, jnp.bfloat16


def normalize(summed, scaling, offset):
    center = summed - jnp.mean(summed, axis=-1, keepdims=True)
    spread = jnp.mean(center * center, axis=-1, keepdims=True)
    return center * lax.rsqrt(spread + norm_eps) * scaling + offset


def half_step(inputs, gate_weight, up_weight, down_weight):
    gate = jnp.dot(inputs, lax.all_gather(gate_weight, "fs", axis=0, tiled=True), preferred_element_type=F32)
    value = jnp.dot(inputs, lax.all_gather(up_weight, "fs", axis=0, tiled=True), preferred_element_type=F32)
    hidden = (jax.nn.silu(gate) * value).astype(BF16)
    partials = jnp.dot(hidden, lax.all_gather(down_weight, "fs", axis=1, tiled=True), preferred_element_type=F32)
    return lax.psum(partials.astype(BF16), "tp")


def per_device_general(
    tokens, mixer_out, gate_first, up_first, down_first, gate_second, up_second, down_second,
    gain_first, bias_first, gain_middle, bias_middle, gain_last, bias_last,
):
    first_branch = half_step(tokens, gate_first, up_first, down_first)
    first_norm = normalize(
        residual_scale * tokens.astype(F32) + 0.5 * first_branch.astype(F32), gain_first, bias_first
    ).astype(BF16)
    middle_norm = normalize(
        residual_scale * first_norm.astype(F32) + mixer_out.astype(F32), gain_middle, bias_middle
    ).astype(BF16)
    second_branch = half_step(middle_norm, gate_second, up_second, down_second)
    return normalize(
        residual_scale * middle_norm.astype(F32) + 0.5 * second_branch.astype(F32), gain_last, bias_last
    ).astype(BF16)


def slot_of(step):
    return step % ZS


STEPS = range(1, ZS)
WAYS = [(way, d, dy) for way in ("up", "dn") for d in STEPS for dy in range(YS)]
MAIN, EXTRA, DOWN = range(3)
GATE_UP = (MAIN, EXTRA)


def kernel(
    tokens_ref, mixer_ref, g1_ref, u1_ref, d1_ref, g2_ref, u2_ref, d2_ref,
    gain1_ref, bias1_ref, gain2_ref, bias2_ref, gain3_ref, bias3_ref,
    out_ref,
    gum, gux, raw, packed, dn, xb, acc, low, high, hid, keep, psend, precv, xsend, xrecv, ysend, yrecv, br, mix, fin,
    zs_send, zs_recv, ys_send, ys_recv, ag_send, ag_recv, rs_send, rs_recv, fin_send, fin_recv, local,
):
    rep, fs, core = lax.axis_index("rep"), lax.axis_index("fs"), lax.axis_index("tp")
    z, y = fs // YS, fs % YS
    quarter = fin.shape[0]
    half = 4 * quarter
    ks = gum.shape[2] // YS
    main = gum.shape[3] // 2
    fold = gux.shape[2] // YS
    extra = gux.shape[3] // 4
    wide = low.shape[1]
    dcols = dn.shape[3]
    own_q, pair_q = rep * YS + y, rep * YS + 1 - y

    pair = {"fs": z * YS + 1 - y}
    other_core = {"tp": 1 - core}
    near = {"rep": lax.rem(rep + core, 2), "fs": z * YS + lax.rem(y + 1 - core, YS)}
    far = {"rep": lax.rem(rep + 1 - core, 2), "fs": z * YS + lax.rem(y + core, YS)}

    def ds(first, count, unit):
        return pl.ds(pl.multiple_of(first, unit), count)

    mine, sib = ds(core * quarter, quarter, quarter), ds((1 - core) * quarter, quarter, quarter)
    weights = ((g1_ref, u1_ref, d1_ref), (g2_ref, u2_ref, d2_ref))

    def pieces(f, q):
        gate, up, down = weights[f]
        rows, mrows, ex_rows = ds(y * ks, ks, ks), ds(q * main, main, main), ds(4 * main + q * extra, extra, 32)
        return (
            (gate.at[:, ds(q * main, main, main)], gum.at[f, 0, rows, pl.ds(0, main)]),
            (up.at[:, ds(q * main, main, main)], gum.at[f, 0, rows, pl.ds(main, main)]),
            (packed.at[f], gux.at[f, 0, ds(y * fold, fold, fold)]),
            (down.at[mrows], dn.at[f, y, pl.ds(0, main)]),
            (down.at[ex_rows], dn.at[f, y, pl.ds(main, extra)]),
        )

    loads = [
        [
            pltpu.make_async_copy(src, dst, local.at[6 * f + i])
            for i, (src, dst) in enumerate([pieces(f, own_q)[i] for i in (0, 1, 3, 4)] + [
                (w.at[:, pl.ds(4 * main, 4 * extra)], raw.at[f, i]) for i, w in enumerate(weights[f][:2])
            ])
        ]
        for f in range(2)
    ]
    token_loads = [
        pltpu.make_async_copy(tokens_ref.at[mine], xb.at[0, pl.ds(0, quarter)], local.at[12]),
        pltpu.make_async_copy(tokens_ref.at[sib], xb.at[0, pl.ds(half, quarter)], local.at[13]),
    ]
    mixer_load = pltpu.make_async_copy(mixer_ref.at[mine], mix, local.at[14])
    for load in loads[0][:2] + loads[0][4:] + token_loads + loads[0][2:4] + loads[1] + [mixer_load]:
        load.start()

    barrier = pltpu.get_barrier_semaphore()

    def greet(target):
        pl.semaphore_signal(barrier, inc=1, device_id=target, device_id_type=pl.DeviceIdType.MESH)

    def plane(dz):
        return {"fs": lax.rem(z + dz + ZS, ZS) * YS + y}

    for target in (near, far, other_core):
        greet(target)

    @pl.when(z < ZS - 1)
    def _():
        greet(plane(1))

    @pl.when(z > 0)
    def _():
        greet(plane(-1))

    inner = jnp.logical_and(z > 0, z < ZS - 1)

    @pl.when(inner)
    def _():
        pl.semaphore_wait(barrier, 5)

    @pl.when(jnp.logical_not(inner))
    def _():
        pl.semaphore_wait(barrier, 4)

    sent = []

    def remote(src, dst, send_sem, recv_sem, target):
        return pltpu.make_async_remote_copy(
            src_ref=src, dst_ref=dst, send_sem=send_sem, recv_sem=recv_sem,
            device_id=target, device_id_type=pl.DeviceIdType.MESH,
        )

    def send(copy):
        copy.start()
        sent.append(copy)

    def pair_copy(f, i):
        src, dst = pieces(f, pair_q)[i]
        return remote(src, dst, ys_send.at[f, i], ys_recv.at[f, i], pair)

    def pair_landing(f, i):
        gate_rows = ds((1 - y) * ks, ks, ks)
        dst = (
            gum.at[f, 0, gate_rows, pl.ds(0, main)], gum.at[f, 0, gate_rows, pl.ds(main, main)],
            gux.at[f, 0, ds((1 - y) * fold, fold, fold)],
            dn.at[f, 1 - y, pl.ds(0, main)], dn.at[f, 1 - y, pl.ds(main, extra)],
        )[i]
        return remote(dst, dst, ys_send.at[f, i], ys_recv.at[f, i], pair)

    def pair_start(f, which):
        for i in which:
            send(pair_copy(f, i))

    def pair_wait(f, which):
        for i in which:
            pair_landing(f, i).wait_recv()

    def z_copy(f, piece, name):
        way, d, dy = name
        ya = lax.rem(y + dy, YS)
        sign = -1 if way == "up" else 1

        def at(n):
            if piece == MAIN:
                return gum.at[f, n, ds(ya * ks, ks, ks)]
            if piece == EXTRA:
                return gux.at[f, n, ds(ya * fold, fold, fold)]
            return dn.at[f, n * YS + ya]

        sems = zs_send.at[f, piece, WAYS.index(name)], zs_recv.at[f, piece, WAYS.index(name)]
        return remote(at(slot_of(sign * (d - 1))), at(slot_of(sign * d)), *sems, plane(-sign))

    def sends_up(d):
        return jnp.logical_and(z >= d - 1, z < ZS - 1)

    def sends_dn(d):
        return jnp.logical_and(z + d - 1 <= ZS - 1, z > 0)

    def gets_up(d):
        return z >= d

    def gets_dn(d):
        return z + d <= ZS - 1

    def own_send(f, which, dy, who=True):
        for way, does in (("up", sends_up), ("dn", sends_dn)):
            @pl.when(jnp.logical_and(does(1), who))
            def _():
                for piece in which:
                    z_copy(f, piece, (way, 1, dy)).start()

    def own_all(f):
        for which in (GATE_UP, (DOWN,)):
            for dy in range(YS):
                own_send(f, which, dy, jnp.logical_not(inner))

    def forward(f, which, d, dys=range(YS)):
        for dy in dys:
            for way, gets, does in (("up", gets_up, sends_up), ("dn", gets_dn, sends_dn)):
                @pl.when(jnp.logical_and(inner, gets(d)))
                def _():
                    for piece in which:
                        z_copy(f, piece, (way, d, dy)).wait_recv()
                        @pl.when(does(d + 1))
                        def _():
                            z_copy(f, piece, (way, d + 1, dy)).start()

    def arrive(f, which, d, dys=range(YS)):
        for way, end in (("up", ZS - 1), ("dn", 0)):
            @pl.when(z == end)
            def _():
                for dy in dys:
                    for piece in which:
                        z_copy(f, piece, (way, d, dy)).wait_recv()

    def pack(f):
        lane = lax.broadcasted_iota(jnp.int32, (fold, 4 * extra), 1)

        def made(q):
            out = None
            for p in range(4):
                part = raw[f, p % 2, (p // 2) * fold:(p // 2 + 1) * fold, :].astype(F32)
                part = pltpu.roll(part, lax.rem(p - q + 4, 4) * extra, axis=1)
                out = part if p == 0 else jnp.where(lane < p * extra, out, part)
            return out.astype(BF16)

        packed[f] = made(pair_q)
        gux[f, 0, ds(y * fold, fold, fold), :] = made(own_q)

    def gather(f, i):
        target = (near, far, far)[i] if i < 3 else other_core
        src = (0, 0, 1)[i] if i < 3 else i - 3
        dst = i + 1 if i < 3 else i + 1
        return remote(
            xb.at[f, pl.ds(src * quarter, quarter)], xb.at[f, pl.ds(dst * quarter, quarter)],
            ag_send.at[f, i], ag_recv.at[f, i], target,
        )

    def gather_start(f):
        send(gather(f, 0))
        send(gather(f, 1))
        if f:
            send(gather(f, 3))

    def gather_near(f):
        gather(f, 0).wait_recv()
        send(gather(f, 2))
        send(gather(f, 4))

    def gather_far(f):
        gather(f, 1).wait_recv()
        send(gather(f, 5))
        gather(f, 2).wait_recv()
        send(gather(f, 6))

    def gather_wait(f):
        for i in range(3 if f else 4, 7):
            gather(f, i).wait_recv()

    step = 2 * quarter

    def gate_up(f, dz, first=False):
        n, zz = lax.rem(dz + ZS, ZS), z + dz
        base = zz * YS * ks

        @pl.loop(0, 4)
        def _(i):
            rows = ds(i * step, step, step)
            folded = [
                jnp.concatenate(
                    [xb[f, rows, ds(base + at * ks + h * fold, fold, fold)] for at in range(YS)], axis=1
                )
                for h in range(2)
            ]
            parts = (
                (acc, jnp.dot(xb[f, rows, ds(base, YS * ks, YS * ks)], gum[f, n], preferred_element_type=F32)),
                (low, jnp.dot(folded[0], gux[f, n, :, :wide], preferred_element_type=F32)),
                (high, jnp.dot(folded[1], gux[f, n, :, 4 * extra - wide:], preferred_element_type=F32)),
            )
            for total, part in parts:
                if first:
                    total[rows, :] = part
                else:
                    total[rows, :] += part

    def at_distance(d, act):
        if d == 0:
            act(0)
            return

        @pl.loop(0, 2)
        def _(i):
            dz = (2 * i - 1) * d

            @pl.when(jnp.logical_and(z + dz >= 0, z + dz < ZS))
            def _():
                act(dz)

    def both(d, act):
        def slots(dz):
            @pl.loop(0, YS)
            def _(ya):
                act(dz, ya)

        at_distance(d, slots)

    def gated(gate, value):
        return gate / (1.0 + jnp.exp(-gate)) * value

    def activate():
        shift = 2 * extra - (4 * extra - wide)
        some = -(-extra // 128) * 128

        @pl.loop(0, 8)
        def _(i):
            rows = ds(i * quarter, quarter, quarter)
            hid[rows, :main] = gated(acc[rows, :main], acc[rows, main:]).astype(BF16)
            rest = low[rows, :] + pltpu.roll(high[rows, :], wide - shift, axis=1)
            value = pltpu.roll(rest, wide - extra, axis=1)
            made = gated(rest[:, :some], value[:, :some])
            hid[rows, main:] = made[:, :extra].astype(BF16)

    def index(dz, ya):
        return lax.rem(dz + ZS, ZS) * YS + ya

    def to_sibling(f, n):
        return remote(psend.at[f, n], precv.at[f, n], rs_send.at[f, 0, n], rs_recv.at[f, 0, n], other_core)

    def to_far(f, n):
        return remote(xsend.at[f, n], xrecv.at[f, n], rs_send.at[f, 1, n], rs_recv.at[f, 1, n], far)

    def to_near(f, n):
        return remote(ysend.at[f, n], yrecv.at[f, n], rs_send.at[f, 2, n], rs_recv.at[f, 2, n], near)

    def down_slot(f, dz, ya):
        n = index(dz, ya)
        psend[f, n] = jnp.dot(hid[half:, :], dn[f, n], preferred_element_type=F32).astype(BF16)
        to_sibling(f, n).start()
        keep[n] = jnp.dot(hid[:half, :], dn[f, n], preferred_element_type=F32)

    def add_cores(f, dz, ya):
        n = index(dz, ya)
        to_sibling(f, n).wait_recv()
        xsend[f, n] = (keep[n, 2 * quarter:, :] + precv[f, n, 2 * quarter:, :].astype(F32)).astype(BF16)
        to_far(f, n).start()
        keep[n, :2 * quarter, :] = keep[n, :2 * quarter, :] + precv[f, n, :2 * quarter, :].astype(F32)

    def add_far(f, dz, ya):
        n = index(dz, ya)
        to_far(f, n).wait_recv()
        ysend[f, n] = (keep[n, quarter:2 * quarter, :] + xrecv[f, n, quarter:, :].astype(F32)).astype(BF16)
        to_near(f, n).start()
        keep[n, :quarter, :] = keep[n, :quarter, :] + xrecv[f, n, :quarter, :].astype(F32)

    def add_near(f, dz, ya):
        n = index(dz, ya)
        to_near(f, n).wait_recv()
        cols = ds(((z + dz) * YS + ya) * dcols, dcols, dcols)
        br[:, cols] = keep[n, :quarter, :] + yrecv[f, n].astype(F32)

    groups = [(d, dy) for d in range(ZS) for dy in range(YS)]

    def reduce(f, extra_work):
        def each(i, act):
            if 0 <= i < len(groups):
                d, dy = groups[i]
                at_distance(d, lambda dz: act(f, dz, lax.rem(y + dy, YS)))

        for i in range(len(groups) + 5):
            if i < len(groups) and groups[i][0]:
                arrive(f, (DOWN,), groups[i][0], (groups[i][1],))
            each(i, down_slot)
            each(i - 1, add_cores)
            each(i - 3, add_far)
            each(i - 5, add_near)
            if i in extra_work:
                extra_work[i]()

    def first_norms():
        @pl.loop(0, quarter // 32)
        def _(i):
            rows = ds(i * 32, 32, 32)
            first = normalize(
                residual_scale * xb[0, rows, :].astype(F32) + 0.5 * br[rows, :], gain1_ref[...], bias1_ref[...]
            ).astype(BF16)
            xb[1, rows, :] = normalize(
                residual_scale * first.astype(F32) + mix[rows, :].astype(F32), gain2_ref[...], bias2_ref[...]
            ).astype(BF16)

    def last_norm():
        @pl.loop(0, quarter // 32)
        def _(i):
            rows = ds(i * 32, 32, 32)
            fin[rows, :] = normalize(
                residual_scale * xb[1, rows, :].astype(F32) + 0.5 * br[rows, :], gain3_ref[...], bias3_ref[...]
            ).astype(BF16)

    def load_wait(f, which):
        for i in which:
            loads[f][i].wait()

    outer = jnp.logical_not(inner)
    pair_start(0, (0, 1))
    load_wait(0, (0, 1))
    own_send(0, (MAIN,), 0)
    load_wait(0, (4, 5))
    pack(0)
    pair_start(0, (2,))
    own_send(0, (EXTRA,), 0)
    token_loads[0].wait()
    gather_start(0)
    pair_start(0, (3, 4))
    load_wait(0, (2, 3))
    own_send(0, (DOWN,), 0)
    load_wait(1, range(6))
    pack(1)
    pair_wait(0, range(3))
    own_send(0, GATE_UP, 1)
    forward(0, GATE_UP, 1, (0,))
    gather_near(0)
    forward(0, GATE_UP, 1, (1,))
    gather_far(0)
    forward(0, GATE_UP, 2, (0,))
    pair_start(1, range(5))
    pair_wait(0, (3, 4))
    own_send(0, (DOWN,), 1, outer)
    token_loads[1].wait()
    gather_wait(0)
    gate_up(0, 0, first=True)
    forward(0, GATE_UP, 2, (1,))
    arrive(0, GATE_UP, 1)
    at_distance(1, lambda dz: gate_up(0, dz))
    own_send(0, (DOWN,), 1, inner)
    arrive(0, GATE_UP, 2)
    at_distance(2, lambda dz: gate_up(0, dz))
    pair_wait(1, range(5))
    own_all(1)
    arrive(0, GATE_UP, 3)
    at_distance(3, lambda dz: gate_up(0, dz))
    activate()
    forward(0, (DOWN,), 1)
    forward(0, (DOWN,), 2)
    own_send(1, GATE_UP, 0, inner)
    own_send(1, GATE_UP, 1, inner)
    reduce(0, {6: lambda: forward(1, GATE_UP, 1)})
    mixer_load.wait()
    first_norms()
    gather_start(1)
    forward(1, GATE_UP, 2)
    own_send(1, (DOWN,), 0, inner)
    own_send(1, (DOWN,), 1, inner)
    gather_near(1)
    forward(1, (DOWN,), 1)
    gather_far(1)
    forward(1, (DOWN,), 2)
    gather_wait(1)
    gate_up(1, 0, first=True)
    arrive(1, GATE_UP, 1)
    at_distance(1, lambda dz: gate_up(1, dz))
    arrive(1, GATE_UP, 2)
    at_distance(2, lambda dz: gate_up(1, dz))
    arrive(1, GATE_UP, 3)
    at_distance(3, lambda dz: gate_up(1, dz))
    activate()
    reduce(1, {})
    last_norm()
    put = pltpu.make_async_copy(fin, out_ref.at[mine], local.at[15])
    put.start()
    over = remote(fin, out_ref.at[mine], fin_send.at[0], fin_recv.at[0], other_core)
    over.start()
    over.wait()
    put.wait()
    for copy in sent:
        copy.wait_send()
    for f in range(2):
        @pl.loop(0, ZS * YS)
        def _(n):
            for copy in (to_sibling(f, n), to_far(f, n), to_near(f, n)):
                copy.wait_send()

        for d in STEPS:
            for way, does in (("up", sends_up), ("dn", sends_dn)):
                @pl.when(does(d))
                def _():
                    for piece in range(3):
                        for dy in range(YS):
                            z_copy(f, piece, (way, d, dy)).wait_send()


def per_device(
    tokens, mixer_out, gate_first, up_first, down_first, gate_second, up_second, down_second,
    gain_first, bias_first, gain_middle, bias_middle, gain_last, bias_last,
):
    rows, width = tokens.shape
    ks, hidden = gate_first.shape
    dcols = down_first.shape[1]
    quarter = rows // 2
    main, extra = split(hidden)
    wide = -(-2 * extra // 128) * 128
    slots = ZS * YS

    any_spec, vmem = pl.BlockSpec(memory_space=pl.ANY), pl.BlockSpec(memory_space=pltpu.VMEM)
    vec = lambda v: v.reshape(1, width)
    dma = pltpu.SemaphoreType.DMA
    return pl.pallas_call(
        kernel,
        out_shape=jax.ShapeDtypeStruct((rows, width), BF16),
        in_specs=[any_spec] * 8 + [vmem] * 6,
        out_specs=any_spec,
        scratch_shapes=[
            pltpu.VMEM((2, ZS, YS * ks, 2 * main), BF16),
            pltpu.VMEM((2, ZS, YS * ks // 2, 4 * extra), BF16),
            pltpu.VMEM((2, 2, ks, 4 * extra), BF16),
            pltpu.VMEM((2, ks // 2, 4 * extra), BF16),
            pltpu.VMEM((2, slots, main + extra, dcols), BF16),
            pltpu.VMEM((2, 8 * quarter, width), BF16),
            pltpu.VMEM((8 * quarter, 2 * main), F32),
            pltpu.VMEM((8 * quarter, wide), F32),
            pltpu.VMEM((8 * quarter, wide), F32),
            pltpu.VMEM((8 * quarter, main + extra), BF16),
            pltpu.VMEM((slots, 4 * quarter, dcols), F32),
            pltpu.VMEM((2, slots, 4 * quarter, dcols), BF16),
            pltpu.VMEM((2, slots, 4 * quarter, dcols), BF16),
            pltpu.VMEM((2, slots, 2 * quarter, dcols), BF16),
            pltpu.VMEM((2, slots, 2 * quarter, dcols), BF16),
            pltpu.VMEM((2, slots, quarter, dcols), BF16),
            pltpu.VMEM((2, slots, quarter, dcols), BF16),
            pltpu.VMEM((quarter, width), F32),
            pltpu.VMEM((quarter, width), BF16),
            pltpu.VMEM((quarter, width), BF16),
            dma((2, 3, len(WAYS))), dma((2, 3, len(WAYS))),
            dma((2, 5)), dma((2, 5)),
            dma((2, 7)), dma((2, 7)),
            dma((2, 3, slots)), dma((2, 3, slots)),
            dma((1,)), dma((1,)),
            dma((16,)),
        ],
        compiler_params=pltpu.CompilerParams(
            collective_id=0, has_side_effects=True, vmem_limit_bytes=60 * 1024 * 1024
        ),
    )(
        tokens, mixer_out,
        gate_first, up_first, down_first, gate_second, up_second, down_second,
        vec(gain_first), vec(bias_first), vec(gain_middle), vec(bias_middle), vec(gain_last), vec(bias_last),
    )


def split(hidden):
    main = hidden // 4 // 128 * 128
    return main, hidden // 4 - main


def on_mesh(mesh, rows, width, hidden):
    sizes = dict(mesh.shape)
    if (sizes["rep"], sizes["fs"], sizes["tp"]) != (2, ZS * YS, 2):
        return False
    rows, ks, hidden = rows // (2 * ZS * YS), width // (ZS * YS), hidden // 2
    main, extra = split(hidden)
    return rows % 32 == 0 and ks % 256 == 0 and hidden % 128 == 0 and main > 0 and extra > 0 and extra % 32 == 0


def solution(mesh):
    def run(tokens, mixer_out, gate_first, *rest):
        fits = on_mesh(mesh, tokens.shape[0], tokens.shape[1], gate_first.shape[1])
        return jax.shard_map(
            per_device if fits else per_device_general,
            mesh=mesh,
            in_specs=(
                P(("rep", "fs"), None), P(("rep", "fs"), None),
                P("fs", "tp"), P("fs", "tp"), P("tp", "fs"),
                P("fs", "tp"), P("fs", "tp"), P("tp", "fs"),
                P(), P(), P(), P(), P(), P(),
            ),
            out_specs=P(("rep", "fs"), None),
            check_vma=False,
        )(tokens, mixer_out, gate_first, *rest)

    return run
```

```python
import math

import jax
import jax.numpy as jnp
from jax import lax
from jax.experimental import pallas as pl
from jax.experimental.pallas import tpu as pltpu
from jax.sharding import PartitionSpec as P

residual_scale = math.sqrt(2.0)
norm_eps = 1e-05
ZS, YS = 4, 2
F32, BF16 = jnp.float32, jnp.bfloat16


def normalize(summed, scaling, offset):
    center = summed - jnp.mean(summed, axis=-1, keepdims=True)
    spread = jnp.mean(center * center, axis=-1, keepdims=True)
    return center * lax.rsqrt(spread + norm_eps) * scaling + offset


def half_step(inputs, gate_weight, up_weight, down_weight):
    gate = jnp.dot(inputs, lax.all_gather(gate_weight, "fs", axis=0, tiled=True), preferred_element_type=F32)
    value = jnp.dot(inputs, lax.all_gather(up_weight, "fs", axis=0, tiled=True), preferred_element_type=F32)
    hidden = (jax.nn.silu(gate) * value).astype(BF16)
    partials = jnp.dot(hidden, lax.all_gather(down_weight, "fs", axis=1, tiled=True), preferred_element_type=F32)
    return lax.psum(partials.astype(BF16), "tp")


def per_device_general(
    tokens, mixer_out, gate_first, up_first, down_first, gate_second, up_second, down_second,
    gain_first, bias_first, gain_middle, bias_middle, gain_last, bias_last,
):
    first_branch = half_step(tokens, gate_first, up_first, down_first)
    first_norm = normalize(
        residual_scale * tokens.astype(F32) + 0.5 * first_branch.astype(F32), gain_first, bias_first
    ).astype(BF16)
    middle_norm = normalize(
        residual_scale * first_norm.astype(F32) + mixer_out.astype(F32), gain_middle, bias_middle
    ).astype(BF16)
    second_branch = half_step(middle_norm, gate_second, up_second, down_second)
    return normalize(
        residual_scale * middle_norm.astype(F32) + 0.5 * second_branch.astype(F32), gain_last, bias_last
    ).astype(BF16)


def slot_of(step):
    return step % ZS


STEPS = range(1, ZS)
WAYS = [(way, d, dy) for way in ("up", "dn") for d in STEPS for dy in range(YS)]
MAIN, EXTRA, DOWN = range(3)
GATE_UP = (MAIN, EXTRA)


FIRST_ORDER = "D0 D1 C0 D2 C1 D3 C2 F0 D4 C3 F1 D5 C4 F2 N0 D6 C5 F3 N1 D7 C6 F4 N2 C7 F5 N3 F6 N4 F7 N5 N6 N7"
LAST_ORDER = "D0 D1 C0 D2 C1 D3 C2 F0 C3 F1 D4 C4 F2 D5 C5 F3 D6 C6 F4 D7 C7 F5 N0 N1 N2 F6 N3 N4 F7 N5 N6 N7"


def kernel(
    tokens_ref, mixer_ref, g1_ref, u1_ref, d1_ref, g2_ref, u2_ref, d2_ref,
    gain1_hbm, bias1_hbm, gain2_hbm, bias2_hbm, gain3_hbm, bias3_hbm,
    out_ref,
    vecs, gum, gux, raw, packed, dn, xb, acc, low, high, hid, keep, psend, precv, xsend, xrecv, ysend, yrecv, br, mix,
    zs_send, zs_recv, ys_send, ys_recv, ag_send, ag_recv, rs_send, rs_recv, fin_send, fin_recv, local,
):
    rep, fs, core = lax.axis_index("rep"), lax.axis_index("fs"), lax.axis_index("tp")
    z, y = fs // YS, fs % YS
    quarter = br.shape[0]
    half = 4 * quarter
    ks = gum.shape[2] // YS
    main = gum.shape[3] // 2
    fold = gux.shape[2] // YS
    extra = gux.shape[3] // 4
    wide = low.shape[1]
    dcols = dn.shape[3]
    own_q, pair_q = rep * YS + y, rep * YS + 1 - y

    pair = {"fs": z * YS + 1 - y}
    other_core = {"tp": 1 - core}
    near = {"rep": lax.rem(rep + core, 2), "fs": z * YS + lax.rem(y + 1 - core, YS)}
    far = {"rep": lax.rem(rep + 1 - core, 2), "fs": z * YS + lax.rem(y + core, YS)}

    def ds(first, count, unit):
        return pl.ds(pl.multiple_of(first, unit), count)

    mine, sib = ds(core * quarter, quarter, quarter), ds((1 - core) * quarter, quarter, quarter)
    weights = ((g1_ref, u1_ref, d1_ref), (g2_ref, u2_ref, d2_ref))

    def pieces(f, q):
        gate, up, down = weights[f]
        rows, mrows, ex_rows = ds(y * ks, ks, ks), ds(q * main, main, main), ds(4 * main + q * extra, extra, 32)
        return (
            (gate.at[:, ds(q * main, main, main)], gum.at[f, 0, rows, pl.ds(0, main)]),
            (up.at[:, ds(q * main, main, main)], gum.at[f, 0, rows, pl.ds(main, main)]),
            (packed.at[f], gux.at[f, 0, ds(y * fold, fold, fold)]),
            (down.at[mrows], dn.at[f, y, pl.ds(0, main)]),
            (down.at[ex_rows], dn.at[f, y, pl.ds(main, extra)]),
        )

    loads = [
        [
            pltpu.make_async_copy(src, dst, local.at[6 * f + i])
            for i, (src, dst) in enumerate([pieces(f, own_q)[i] for i in (0, 1, 3, 4)] + [
                (w.at[:, pl.ds(4 * main, 4 * extra)], raw.at[f, i]) for i, w in enumerate(weights[f][:2])
            ])
        ]
        for f in range(2)
    ]
    token_loads = [
        pltpu.make_async_copy(tokens_ref.at[mine], xb.at[0, pl.ds(0, quarter)], local.at[12]),
        pltpu.make_async_copy(tokens_ref.at[sib], xb.at[0, pl.ds(half, quarter)], local.at[13]),
    ]
    vec_loads = [
        pltpu.make_async_copy(src, vecs.at[i], local.at[15 + i])
        for i, src in enumerate((gain1_hbm, bias1_hbm, gain2_hbm, bias2_hbm, gain3_hbm, bias3_hbm))
    ]
    mixer_load = pltpu.make_async_copy(mixer_ref.at[mine], mix, local.at[14])
    for load in loads[0][:2] + loads[0][4:] + token_loads + loads[0][2:4] + loads[1] + [mixer_load] + vec_loads:
        load.start()

    barrier = pltpu.get_barrier_semaphore()

    def greet(target):
        pl.semaphore_signal(barrier, inc=1, device_id=target, device_id_type=pl.DeviceIdType.MESH)

    def plane(dz):
        return {"fs": lax.rem(z + dz + ZS, ZS) * YS + y}

    for target in (near, far, other_core):
        greet(target)

    @pl.when(z < ZS - 1)
    def _():
        greet(plane(1))

    @pl.when(z > 0)
    def _():
        greet(plane(-1))

    inner = jnp.logical_and(z > 0, z < ZS - 1)

    @pl.when(inner)
    def _():
        pl.semaphore_wait(barrier, 5)

    @pl.when(jnp.logical_not(inner))
    def _():
        pl.semaphore_wait(barrier, 4)

    sent = []

    def remote(src, dst, send_sem, recv_sem, target):
        return pltpu.make_async_remote_copy(
            src_ref=src, dst_ref=dst, send_sem=send_sem, recv_sem=recv_sem,
            device_id=target, device_id_type=pl.DeviceIdType.MESH,
        )

    def send(copy):
        copy.start()
        sent.append(copy)

    def pair_copy(f, i):
        src, dst = pieces(f, pair_q)[i]
        return remote(src, dst, ys_send.at[f, i], ys_recv.at[f, i], pair)

    def pair_landing(f, i):
        gate_rows = ds((1 - y) * ks, ks, ks)
        dst = (
            gum.at[f, 0, gate_rows, pl.ds(0, main)], gum.at[f, 0, gate_rows, pl.ds(main, main)],
            gux.at[f, 0, ds((1 - y) * fold, fold, fold)],
            dn.at[f, 1 - y, pl.ds(0, main)], dn.at[f, 1 - y, pl.ds(main, extra)],
        )[i]
        return remote(dst, dst, ys_send.at[f, i], ys_recv.at[f, i], pair)

    def pair_start(f, which):
        for i in which:
            send(pair_copy(f, i))

    def pair_wait(f, which):
        for i in which:
            pair_landing(f, i).wait_recv()

    def z_copy(f, piece, name):
        way, d, dy = name
        ya = lax.rem(y + dy, YS)
        sign = -1 if way == "up" else 1

        def at(n):
            if piece == MAIN:
                return gum.at[f, n, ds(ya * ks, ks, ks)]
            if piece == EXTRA:
                return gux.at[f, n, ds(ya * fold, fold, fold)]
            return dn.at[f, n * YS + ya]

        sems = zs_send.at[f, piece, WAYS.index(name)], zs_recv.at[f, piece, WAYS.index(name)]
        return remote(at(slot_of(sign * (d - 1))), at(slot_of(sign * d)), *sems, plane(-sign))

    def sends_up(d):
        return jnp.logical_and(z >= d - 1, z < ZS - 1)

    def sends_dn(d):
        return jnp.logical_and(z + d - 1 <= ZS - 1, z > 0)

    def gets_up(d):
        return z >= d

    def gets_dn(d):
        return z + d <= ZS - 1

    def own_send(f, which, dy, who=True):
        for way, does in (("up", sends_up), ("dn", sends_dn)):
            @pl.when(jnp.logical_and(does(1), who))
            def _():
                for piece in which:
                    z_copy(f, piece, (way, 1, dy)).start()

    def own_all(f):
        for which in (GATE_UP, (DOWN,)):
            for dy in range(YS):
                own_send(f, which, dy, jnp.logical_not(inner))

    def forward(f, which, d, dys=range(YS)):
        for dy in dys:
            for way, gets, does in (("up", gets_up, sends_up), ("dn", gets_dn, sends_dn)):
                @pl.when(jnp.logical_and(inner, gets(d)))
                def _():
                    for piece in which:
                        z_copy(f, piece, (way, d, dy)).wait_recv()
                        @pl.when(does(d + 1))
                        def _():
                            z_copy(f, piece, (way, d + 1, dy)).start()

    def arrive(f, which, d, dys=range(YS)):
        for way, end in (("up", ZS - 1), ("dn", 0)):
            @pl.when(z == end)
            def _():
                for dy in dys:
                    for piece in which:
                        z_copy(f, piece, (way, d, dy)).wait_recv()

    def pack(f):
        lane = lax.broadcasted_iota(jnp.int32, (fold, 4 * extra), 1)

        def made(q):
            out = None
            for p in range(4):
                part = raw[f, p % 2, (p // 2) * fold:(p // 2 + 1) * fold, :].astype(F32)
                part = pltpu.roll(part, lax.rem(p - q + 4, 4) * extra, axis=1)
                out = part if p == 0 else jnp.where(lane < p * extra, out, part)
            return out.astype(BF16)

        packed[f] = made(pair_q)
        gux[f, 0, ds(y * fold, fold, fold), :] = made(own_q)

    def gather(f, i):
        target = (near, far, far)[i] if i < 3 else other_core
        src = (0, 0, 1)[i] if i < 3 else i - 3
        dst = i + 1 if i < 3 else i + 1
        return remote(
            xb.at[f, pl.ds(src * quarter, quarter)], xb.at[f, pl.ds(dst * quarter, quarter)],
            ag_send.at[f, i], ag_recv.at[f, i], target,
        )

    def gather_start(f):
        send(gather(f, 0))
        send(gather(f, 1))
        if f:
            send(gather(f, 3))

    def gather_near(f):
        gather(f, 0).wait_recv()
        send(gather(f, 2))
        send(gather(f, 4))

    def gather_far(f):
        gather(f, 1).wait_recv()
        send(gather(f, 5))
        gather(f, 2).wait_recv()
        send(gather(f, 6))

    def gather_wait(f):
        for i in range(3 if f else 4, 7):
            gather(f, i).wait_recv()

    step = 2 * quarter

    def gate_up(f, dz, first=False):
        n, zz = lax.rem(dz + ZS, ZS), z + dz
        base = zz * YS * ks

        @pl.loop(0, 4)
        def _(i):
            rows = ds(i * step, step, step)
            folded = [
                jnp.concatenate(
                    [xb[f, rows, ds(base + at * ks + h * fold, fold, fold)] for at in range(YS)], axis=1
                )
                for h in range(2)
            ]
            parts = (
                (acc, jnp.dot(xb[f, rows, ds(base, YS * ks, YS * ks)], gum[f, n], preferred_element_type=F32)),
                (low, jnp.dot(folded[0], gux[f, n, :, :wide], preferred_element_type=F32)),
                (high, jnp.dot(folded[1], gux[f, n, :, 4 * extra - wide:], preferred_element_type=F32)),
            )
            for total, part in parts:
                if first:
                    total[rows, :] = part
                else:
                    total[rows, :] += part

    def at_distance(d, act):
        if d == 0:
            act(0)
            return

        @pl.loop(0, 2)
        def _(i):
            dz = (2 * i - 1) * d

            @pl.when(jnp.logical_and(z + dz >= 0, z + dz < ZS))
            def _():
                act(dz)

    def both(d, act):
        def slots(dz):
            @pl.loop(0, YS)
            def _(ya):
                act(dz, ya)

        at_distance(d, slots)

    def gated(gate, value):
        return gate / (1.0 + jnp.exp(-gate)) * value

    def activate():
        shift = 2 * extra - (4 * extra - wide)
        some = -(-extra // 128) * 128

        @pl.loop(0, 8)
        def _(i):
            rows = ds(i * quarter, quarter, quarter)
            hid[rows, :main] = gated(acc[rows, :main], acc[rows, main:]).astype(BF16)
            rest = low[rows, :] + pltpu.roll(high[rows, :], wide - shift, axis=1)
            value = pltpu.roll(rest, wide - extra, axis=1)
            made = gated(rest[:, :some], value[:, :some])
            hid[rows, main:] = made[:, :extra].astype(BF16)

    def index(dz, ya):
        return lax.rem(dz + ZS, ZS) * YS + ya

    def to_sibling(f, n):
        return remote(psend.at[f, n], precv.at[f, n], rs_send.at[f, 0, n], rs_recv.at[f, 0, n], other_core)

    def to_far(f, n):
        return remote(xsend.at[f, n], xrecv.at[f, n], rs_send.at[f, 1, n], rs_recv.at[f, 1, n], far)

    def to_near(f, n):
        return remote(ysend.at[f, n], yrecv.at[f, n], rs_send.at[f, 2, n], rs_recv.at[f, 2, n], near)

    def down_slot(f, dz, ya):
        n = index(dz, ya)
        psend[f, n] = jnp.dot(hid[half:, :], dn[f, n], preferred_element_type=F32).astype(BF16)
        to_sibling(f, n).start()
        keep[n] = jnp.dot(hid[:half, :], dn[f, n], preferred_element_type=F32)

    def add_cores(f, dz, ya):
        n = index(dz, ya)
        to_sibling(f, n).wait_recv()
        xsend[f, n] = (keep[n, 2 * quarter:, :] + precv[f, n, 2 * quarter:, :].astype(F32)).astype(BF16)
        to_far(f, n).start()
        keep[n, :2 * quarter, :] = keep[n, :2 * quarter, :] + precv[f, n, :2 * quarter, :].astype(F32)

    def add_far(f, dz, ya):
        n = index(dz, ya)
        to_far(f, n).wait_recv()
        ysend[f, n] = (keep[n, quarter:2 * quarter, :] + xrecv[f, n, quarter:, :].astype(F32)).astype(BF16)
        to_near(f, n).start()
        keep[n, :quarter, :] = keep[n, :quarter, :] + xrecv[f, n, :quarter, :].astype(F32)

    def add_near(f, dz, ya):
        n = index(dz, ya)
        to_near(f, n).wait_recv()
        cols = ds(((z + dz) * YS + ya) * dcols, dcols, dcols)
        br[:, cols] = keep[n, :quarter, :] + yrecv[f, n].astype(F32)

    groups = [(d, dy) for d in range(ZS) for dy in range(YS)]

    stages = {"C": add_cores, "F": add_far, "N": add_near}

    def reduce(f, order, extra_work):
        for i, name in enumerate(order.split()):
            d, dy = groups[int(name[1])]
            act = stages.get(name[0], down_slot)
            if act is down_slot and d:
                arrive(f, (DOWN,), d, (dy,))
            at_distance(d, lambda dz: act(f, dz, lax.rem(y + dy, YS)))
            if name in extra_work:
                extra_work[name]()

    def first_norms():
        @pl.loop(0, quarter // 32)
        def _(i):
            rows = ds(i * 32, 32, 32)
            first = normalize(
                residual_scale * xb[0, rows, :].astype(F32) + 0.5 * br[rows, :], vecs[0], vecs[1]
            ).astype(BF16)
            xb[1, rows, :] = normalize(
                residual_scale * first.astype(F32) + mix[rows, :].astype(F32), vecs[2], vecs[3]
            ).astype(BF16)

    def out_copy(i):
        rows = ds(core * quarter + i * 32, 32, 32)
        return remote(out_ref.at[rows], out_ref.at[rows], fin_send.at[i], fin_recv.at[i], other_core)

    def last_norm():
        @pl.loop(0, quarter // 32)
        def _(i):
            rows = ds(i * 32, 32, 32)
            out_ref[ds(core * quarter + i * 32, 32, 32), :] = normalize(
                residual_scale * xb[1, rows, :].astype(F32) + 0.5 * br[rows, :], vecs[4], vecs[5]
            ).astype(BF16)
            out_copy(i).start()

    def sent_wait():
        for copy in sent:
            copy.wait_send()
        sent.clear()

    def z_sent_wait(f):
        for d in STEPS:
            for way, does in (("up", sends_up), ("dn", sends_dn)):
                @pl.when(does(d))
                def _():
                    for piece in range(3):
                        for dy in range(YS):
                            z_copy(f, piece, (way, d, dy)).wait_send()

    def reduce_sent_wait(f):
        @pl.loop(0, ZS * YS)
        def _(n):
            for copy in (to_sibling(f, n), to_far(f, n), to_near(f, n)):
                copy.wait_send()

    def load_wait(f, which):
        for i in which:
            loads[f][i].wait()

    outer = jnp.logical_not(inner)

    def outer_middle():
        @pl.when(outer)
        def _():
            pair_wait(1, range(5))

        own_all(1)

    def inner_middle():
        forward(0, (DOWN,), 2)

        @pl.when(inner)
        def _():
            pair_wait(1, range(5))

        own_send(1, GATE_UP, 0, inner)
        own_send(1, GATE_UP, 1, inner)

    pair_start(0, (0, 1))
    load_wait(0, (0, 1))
    own_send(0, (MAIN,), 0)
    load_wait(0, (4, 5))
    pack(0)
    pair_start(0, (2,))
    own_send(0, (EXTRA,), 0)
    token_loads[0].wait()
    gather_start(0)
    pair_start(0, (3, 4))
    load_wait(0, (2, 3))
    own_send(0, (DOWN,), 0)
    load_wait(1, range(6))
    pack(1)
    pair_wait(0, range(3))
    own_send(0, GATE_UP, 1)
    forward(0, GATE_UP, 1, (0,))
    gather_near(0)
    forward(0, GATE_UP, 1, (1,))
    gather_far(0)
    forward(0, GATE_UP, 2, (0,))
    pair_start(1, range(5))
    pair_wait(0, (3, 4))
    own_send(0, (DOWN,), 1, outer)
    token_loads[1].wait()
    gather_wait(0)
    gate_up(0, 0, first=True)
    forward(0, GATE_UP, 2, (1,))
    arrive(0, GATE_UP, 1)
    at_distance(1, lambda dz: gate_up(0, dz))
    own_send(0, (DOWN,), 1, inner)
    arrive(0, GATE_UP, 2)
    at_distance(2, lambda dz: gate_up(0, dz))
    outer_middle()
    arrive(0, GATE_UP, 3)
    at_distance(3, lambda dz: gate_up(0, dz))
    activate()
    forward(0, (DOWN,), 1)
    reduce(0, FIRST_ORDER, {"D3": inner_middle, "F3": lambda: forward(1, GATE_UP, 1)})
    for load in [mixer_load] + vec_loads:
        load.wait()
    first_norms()
    gather_start(1)
    gather_near(1)
    forward(1, GATE_UP, 2)
    own_send(1, (DOWN,), 0, inner)
    own_send(1, (DOWN,), 1, inner)
    gather_far(1)
    gather_wait(1)
    gate_up(1, 0, first=True)
    forward(1, (DOWN,), 1)
    arrive(1, GATE_UP, 1)
    at_distance(1, lambda dz: gate_up(1, dz))
    forward(1, (DOWN,), 2)
    arrive(1, GATE_UP, 2)
    at_distance(2, lambda dz: gate_up(1, dz))
    sent_wait()
    z_sent_wait(0)
    reduce_sent_wait(0)
    arrive(1, GATE_UP, 3)
    at_distance(3, lambda dz: gate_up(1, dz))
    activate()
    reduce(1, LAST_ORDER, {"F7": lambda: z_sent_wait(1)})
    reduce_sent_wait(1)
    last_norm()
    @pl.loop(0, quarter // 32)
    def _(i):
        out_copy(i).wait()


def per_device(
    tokens, mixer_out, gate_first, up_first, down_first, gate_second, up_second, down_second,
    gain_first, bias_first, gain_middle, bias_middle, gain_last, bias_last,
):
    rows, width = tokens.shape
    ks, hidden = gate_first.shape
    dcols = down_first.shape[1]
    quarter = rows // 2
    main, extra = split(hidden)
    wide = -(-2 * extra // 128) * 128
    slots = ZS * YS

    any_spec, vmem = pl.BlockSpec(memory_space=pl.ANY), pl.BlockSpec(memory_space=pltpu.VMEM)
    vec = lambda v: v.reshape(1, width)
    dma = pltpu.SemaphoreType.DMA
    return pl.pallas_call(
        kernel,
        out_shape=pltpu.VMEM((rows, width), BF16),
        in_specs=[any_spec] * 14,
        out_specs=pl.BlockSpec(memory_space=pltpu.VMEM),
        scratch_shapes=[
            pltpu.VMEM((6, 1, width), F32),
            pltpu.VMEM((2, ZS, YS * ks, 2 * main), BF16),
            pltpu.VMEM((2, ZS, YS * ks // 2, 4 * extra), BF16),
            pltpu.VMEM((2, 2, ks, 4 * extra), BF16),
            pltpu.VMEM((2, ks // 2, 4 * extra), BF16),
            pltpu.VMEM((2, slots, main + extra, dcols), BF16),
            pltpu.VMEM((2, 8 * quarter, width), BF16),
            pltpu.VMEM((8 * quarter, 2 * main), F32),
            pltpu.VMEM((8 * quarter, wide), F32),
            pltpu.VMEM((8 * quarter, wide), F32),
            pltpu.VMEM((8 * quarter, main + extra), BF16),
            pltpu.VMEM((slots, 4 * quarter, dcols), F32),
            pltpu.VMEM((2, slots, 4 * quarter, dcols), BF16),
            pltpu.VMEM((2, slots, 4 * quarter, dcols), BF16),
            pltpu.VMEM((2, slots, 2 * quarter, dcols), BF16),
            pltpu.VMEM((2, slots, 2 * quarter, dcols), BF16),
            pltpu.VMEM((2, slots, quarter, dcols), BF16),
            pltpu.VMEM((2, slots, quarter, dcols), BF16),
            pltpu.VMEM((quarter, width), F32),
            pltpu.VMEM((quarter, width), BF16),
            dma((2, 3, len(WAYS))), dma((2, 3, len(WAYS))),
            dma((2, 5)), dma((2, 5)),
            dma((2, 7)), dma((2, 7)),
            dma((2, 3, slots)), dma((2, 3, slots)),
            dma((quarter // 32,)), dma((quarter // 32,)),
            dma((21,)),
        ],
        compiler_params=pltpu.CompilerParams(
            collective_id=0, has_side_effects=True, vmem_limit_bytes=60 * 1024 * 1024
        ),
    )(
        tokens, mixer_out,
        gate_first, up_first, down_first, gate_second, up_second, down_second,
        vec(gain_first), vec(bias_first), vec(gain_middle), vec(bias_middle), vec(gain_last), vec(bias_last),
    )


def split(hidden):
    main = hidden // 4 // 128 * 128
    return main, hidden // 4 - main


def on_mesh(mesh, rows, width, hidden):
    sizes = dict(mesh.shape)
    if (sizes["rep"], sizes["fs"], sizes["tp"]) != (2, ZS * YS, 2):
        return False
    rows, ks, hidden = rows // (2 * ZS * YS), width // (ZS * YS), hidden // 2
    main, extra = split(hidden)
    return rows % 32 == 0 and ks % 256 == 0 and hidden % 128 == 0 and main > 0 and extra > 0 and extra % 32 == 0


def solution(mesh):
    def run(tokens, mixer_out, gate_first, *rest):
        fits = on_mesh(mesh, tokens.shape[0], tokens.shape[1], gate_first.shape[1])
        return jax.shard_map(
            per_device if fits else per_device_general,
            mesh=mesh,
            in_specs=(
                P(("rep", "fs"), None), P(("rep", "fs"), None),
                P("fs", "tp"), P("fs", "tp"), P("tp", "fs"),
                P("fs", "tp"), P("fs", "tp"), P("tp", "fs"),
                P(), P(), P(), P(), P(), P(),
            ),
            out_specs=P(("rep", "fs"), None),
            check_vma=False,
        )(tokens, mixer_out, gate_first, *rest)

    return run
```

```python
import math

import jax
import jax.numpy as jnp
from jax import lax
from jax.experimental import pallas as pl
from jax.experimental.pallas import tpu as pltpu
from jax.sharding import PartitionSpec as P

residual_scale = math.sqrt(2.0)
norm_eps = 1e-05
ZS, YS = 4, 2
F32, BF16 = jnp.float32, jnp.bfloat16


def normalize(summed, scaling, offset):
    center = summed - jnp.mean(summed, axis=-1, keepdims=True)
    spread = jnp.mean(center * center, axis=-1, keepdims=True)
    return center * lax.rsqrt(spread + norm_eps) * scaling + offset


def half_step(inputs, gate_weight, up_weight, down_weight):
    gate = jnp.dot(inputs, lax.all_gather(gate_weight, "fs", axis=0, tiled=True), preferred_element_type=F32)
    value = jnp.dot(inputs, lax.all_gather(up_weight, "fs", axis=0, tiled=True), preferred_element_type=F32)
    hidden = (jax.nn.silu(gate) * value).astype(BF16)
    partials = jnp.dot(hidden, lax.all_gather(down_weight, "fs", axis=1, tiled=True), preferred_element_type=F32)
    return lax.psum(partials.astype(BF16), "tp")


def per_device_general(
    tokens, mixer_out, gate_first, up_first, down_first, gate_second, up_second, down_second,
    gain_first, bias_first, gain_middle, bias_middle, gain_last, bias_last,
):
    first_branch = half_step(tokens, gate_first, up_first, down_first)
    first_norm = normalize(
        residual_scale * tokens.astype(F32) + 0.5 * first_branch.astype(F32), gain_first, bias_first
    ).astype(BF16)
    middle_norm = normalize(
        residual_scale * first_norm.astype(F32) + mixer_out.astype(F32), gain_middle, bias_middle
    ).astype(BF16)
    second_branch = half_step(middle_norm, gate_second, up_second, down_second)
    return normalize(
        residual_scale * middle_norm.astype(F32) + 0.5 * second_branch.astype(F32), gain_last, bias_last
    ).astype(BF16)


def slot_of(step):
    return step % ZS


STEPS = range(1, ZS)
MAIN, EXTRA, DOWN = range(3)
GATE_UP = (MAIN, EXTRA)


FIRST_ORDER = "D0 D1 C0 D2 C1 D3 C2 F0 D4 C3 F1 D5 C4 F2 N0 D6 C5 F3 N1 D7 C6 F4 N2 C7 F5 N3 F6 N4 F7 N5 N6 N7"
LAST_ORDER = "D0 D1 C0 D2 C1 D3 C2 F0 C3 F1 D4 C4 F2 D5 C5 F3 D6 C6 F4 D7 C7 F5 N0 N1 N2 F6 N3 N4 F7 N5 N6 N7"


def kernel(
    tokens_ref, mixer_ref, g1_ref, u1_ref, d1_ref, g2_ref, u2_ref, d2_ref,
    gain1_hbm, bias1_hbm, gain2_hbm, bias2_hbm, gain3_hbm, bias3_hbm,
    out_ref,
    vecs, gum, gux, raw, packed, dn, xb, acc, low, high, hid, keep, psend, precv, xsend, xrecv, ysend, yrecv, br, mix,
    zs_send, zs_recv, ys_send, ys_recv, ag_send, ag_recv, rs_send, rs_recv, fin_sem, local,
):
    rep, fs, core = lax.axis_index("rep"), lax.axis_index("fs"), lax.axis_index("tp")
    z, y = fs // YS, fs % YS
    quarter = br.shape[0]
    half = 4 * quarter
    ks = gum.shape[2] // YS
    main = gum.shape[3] // 2
    fold = gux.shape[2] // YS
    extra = gux.shape[3] // 4
    wide = low.shape[1]
    dcols = dn.shape[3]
    own_q, pair_q = rep * YS + y, rep * YS + 1 - y

    pair = {"fs": z * YS + 1 - y}
    other_core = {"tp": 1 - core}
    near = {"rep": lax.rem(rep + core, 2), "fs": z * YS + lax.rem(y + 1 - core, YS)}
    far = {"rep": lax.rem(rep + 1 - core, 2), "fs": z * YS + lax.rem(y + core, YS)}

    def ds(first, count, unit):
        return pl.ds(pl.multiple_of(first, unit), count)

    mine, sib = ds(core * quarter, quarter, quarter), ds((1 - core) * quarter, quarter, quarter)
    weights = ((g1_ref, u1_ref, d1_ref), (g2_ref, u2_ref, d2_ref))

    def pieces(f, q):
        gate, up, down = weights[f]
        rows, mrows, ex_rows = ds(y * ks, ks, ks), ds(q * main, main, main), ds(4 * main + q * extra, extra, 32)
        return (
            (gate.at[:, ds(q * main, main, main)], gum.at[f, 0, rows, pl.ds(0, main)]),
            (up.at[:, ds(q * main, main, main)], gum.at[f, 0, rows, pl.ds(main, main)]),
            (packed.at[f], gux.at[f, 0, ds(y * fold, fold, fold)]),
            (down.at[mrows], dn.at[f, y, pl.ds(0, main)]),
            (down.at[ex_rows], dn.at[f, y, pl.ds(main, extra)]),
        )

    loads = [
        [
            pltpu.make_async_copy(src, dst, local.at[3 * f + i // 2])
            for i, (src, dst) in enumerate([pieces(f, own_q)[i] for i in (0, 1, 3, 4)] + [
                (w.at[:, pl.ds(4 * main, 4 * extra)], raw.at[f, i]) for i, w in enumerate(weights[f][:2])
            ])
        ]
        for f in range(2)
    ]
    token_loads = [
        pltpu.make_async_copy(tokens_ref.at[mine], xb.at[0, pl.ds(0, quarter)], local.at[6]),
        pltpu.make_async_copy(tokens_ref.at[sib], xb.at[0, pl.ds(half, quarter)], local.at[7]),
    ]
    vec_loads = [
        pltpu.make_async_copy(src, vecs.at[i], local.at[9 + i])
        for i, src in enumerate((gain1_hbm, bias1_hbm, gain2_hbm, bias2_hbm, gain3_hbm, bias3_hbm))
    ]
    mixer_load = pltpu.make_async_copy(mixer_ref.at[mine], mix, local.at[8])
    for load in loads[0][:2] + loads[0][4:] + token_loads + loads[0][2:4] + loads[1] + [mixer_load] + vec_loads:
        load.start()

    barrier = pltpu.get_barrier_semaphore()

    def greet(target):
        pl.semaphore_signal(barrier, inc=1, device_id=target, device_id_type=pl.DeviceIdType.MESH)

    def plane(dz):
        return {"fs": lax.rem(z + dz + ZS, ZS) * YS + y}

    for target in (near, far, other_core):
        greet(target)

    @pl.when(z < ZS - 1)
    def _():
        greet(plane(1))

    @pl.when(z > 0)
    def _():
        greet(plane(-1))

    inner = jnp.logical_and(z > 0, z < ZS - 1)

    @pl.when(inner)
    def _():
        pl.semaphore_wait(barrier, 5)

    @pl.when(jnp.logical_not(inner))
    def _():
        pl.semaphore_wait(barrier, 4)

    def remote(src, dst, send_sem, recv_sem, target):
        return pltpu.make_async_remote_copy(
            src_ref=src, dst_ref=dst, send_sem=send_sem, recv_sem=recv_sem,
            device_id=target, device_id_type=pl.DeviceIdType.MESH,
        )

    def pair_copy(f, i):
        src, dst = pieces(f, pair_q)[i]
        n = (0, 0, 1, 2, 2)[i]
        return remote(src, dst, ys_send.at[f, n], ys_recv.at[f, n], pair)

    def pair_landing(f, i):
        dst = (
            gum.at[f, 0, ds((1 - y) * ks, ks, ks)], gux.at[f, 0, ds((1 - y) * fold, fold, fold)], dn.at[f, 1 - y],
        )[i]
        return remote(dst, dst, ys_send.at[f, i], ys_recv.at[f, i], pair)

    def pair_start(f, which):
        for i in which:
            pair_copy(f, i).start()

    def pair_wait(f, which):
        for i in which:
            pair_landing(f, i).wait_recv()

    def z_copy(f, piece, name):
        way, d, dy = name
        ya = lax.rem(y + dy, YS)
        sign = -1 if way == "up" else 1

        def at(n):
            if piece == MAIN:
                return gum.at[f, n, ds(ya * ks, ks, ks)]
            if piece == EXTRA:
                return gux.at[f, n, ds(ya * fold, fold, fold)]
            return dn.at[f, n * YS + ya]

        there = slot_of(sign * d)
        sems = zs_send.at[f, piece, int(way == "up")], zs_recv.at[f, int(piece == DOWN), there - 1, dy]
        return remote(at(slot_of(sign * (d - 1))), at(there), *sems, plane(-sign))

    def z_wait(f, which, name):
        way, d, dy = name
        n = slot_of(-d if way == "up" else d)
        span = (ks * 2 * main + fold * 4 * extra) // xb.shape[2]
        landed = dn.at[f, n * YS] if which == (DOWN,) else xb.at[f, pl.ds(0, span)]
        sem = zs_recv.at[f, int(which == (DOWN,)), n - 1, dy]
        remote(landed, landed, sem, sem, other_core).wait_recv()

    def sends_up(d):
        return jnp.logical_and(z >= d - 1, z < ZS - 1)

    def sends_dn(d):
        return jnp.logical_and(z + d - 1 <= ZS - 1, z > 0)

    def gets_up(d):
        return z >= d

    def gets_dn(d):
        return z + d <= ZS - 1

    def own_send(f, which, dy, who=True):
        for way, does in (("up", sends_up), ("dn", sends_dn)):
            @pl.when(jnp.logical_and(does(1), who))
            def _():
                for piece in which:
                    z_copy(f, piece, (way, 1, dy)).start()

    def own_all(f):
        for which in (GATE_UP, (DOWN,)):
            for dy in range(YS):
                own_send(f, which, dy, jnp.logical_not(inner))

    def forward(f, which, d, dys=range(YS)):
        for dy in dys:
            for way, gets, does in (("up", gets_up, sends_up), ("dn", gets_dn, sends_dn)):
                @pl.when(jnp.logical_and(inner, gets(d)))
                def _():
                    z_wait(f, which, (way, d, dy))

                    @pl.when(does(d + 1))
                    def _():
                        for piece in which:
                            z_copy(f, piece, (way, d + 1, dy)).start()

    def arrive(f, which, d, dys=range(YS)):
        for way, end in (("up", ZS - 1), ("dn", 0)):
            @pl.when(z == end)
            def _():
                for dy in dys:
                    z_wait(f, which, (way, d, dy))

    def pack(f):
        lane = lax.broadcasted_iota(jnp.int32, (fold, 4 * extra), 1)

        def made(q):
            out = None
            for p in range(4):
                part = raw[f, p % 2, (p // 2) * fold:(p // 2 + 1) * fold, :].astype(F32)
                part = pltpu.roll(part, lax.rem(p - q + 4, 4) * extra, axis=1)
                out = part if p == 0 else jnp.where(lane < p * extra, out, part)
            return out.astype(BF16)

        packed[f] = made(pair_q)
        gux[f, 0, ds(y * fold, fold, fold), :] = made(own_q)

    def gather(f, i):
        target = (near, far, far)[i] if i < 3 else other_core
        src = (0, 0, 1)[i] if i < 3 else i - 3
        dst = i + 1 if i < 3 else i + 1
        return remote(
            xb.at[f, pl.ds(src * quarter, quarter)], xb.at[f, pl.ds(dst * quarter, quarter)],
            ag_send.at[0], ag_recv.at[i], target,
        )

    def gather_send(f, i):
        gather(f, i).start()

    def gather_sent_wait(f):
        gone = xb.at[f, pl.ds(0, (6 + f) * quarter)]
        remote(gone, gone, ag_send.at[0], ag_recv.at[0], other_core).wait_send()

    def gather_start(f):
        gather_send(f, 0)
        gather_send(f, 1)
        if f:
            gather_send(f, 3)

    def gather_near(f):
        gather(f, 0).wait_recv()
        gather_send(f, 2)
        gather_send(f, 4)

    def gather_far(f):
        gather(f, 1).wait_recv()
        gather_send(f, 5)
        gather(f, 2).wait_recv()
        gather_send(f, 6)

    def gather_wait(f):
        for i in range(3 if f else 4, 7):
            gather(f, i).wait_recv()

    step = 2 * quarter

    def gate_up(f, dz, first=False):
        n, zz = lax.rem(dz + ZS, ZS), z + dz
        base = zz * YS * ks

        @pl.loop(0, 4)
        def _(i):
            rows = ds(i * step, step, step)
            folded = [
                jnp.concatenate(
                    [xb[f, rows, ds(base + at * ks + h * fold, fold, fold)] for at in range(YS)], axis=1
                )
                for h in range(2)
            ]
            parts = (
                (acc, jnp.dot(xb[f, rows, ds(base, YS * ks, YS * ks)], gum[f, n], preferred_element_type=F32)),
                (low, jnp.dot(folded[0], gux[f, n, :, :wide], preferred_element_type=F32)),
                (high, jnp.dot(folded[1], gux[f, n, :, 4 * extra - wide:], preferred_element_type=F32)),
            )
            for total, part in parts:
                if first:
                    total[rows, :] = part
                else:
                    total[rows, :] += part

    def at_distance(d, act):
        if d == 0:
            act(0)
            return

        @pl.loop(0, 2)
        def _(i):
            dz = (2 * i - 1) * d

            @pl.when(jnp.logical_and(z + dz >= 0, z + dz < ZS))
            def _():
                act(dz)

    def both(d, act):
        def slots(dz):
            @pl.loop(0, YS)
            def _(ya):
                act(dz, ya)

        at_distance(d, slots)

    def gated(gate, value):
        return gate / (1.0 + jnp.exp(-gate)) * value

    def activate():
        shift = 2 * extra - (4 * extra - wide)
        some = -(-extra // 128) * 128

        @pl.loop(0, 8)
        def _(i):
            rows = ds(i * quarter, quarter, quarter)
            hid[rows, :main] = gated(acc[rows, :main], acc[rows, main:]).astype(BF16)
            rest = low[rows, :] + pltpu.roll(high[rows, :], wide - shift, axis=1)
            value = pltpu.roll(rest, wide - extra, axis=1)
            made = gated(rest[:, :some], value[:, :some])
            hid[rows, main:] = made[:, :extra].astype(BF16)

    def index(dz, ya):
        return lax.rem(dz + ZS, ZS) * YS + ya

    def to_sibling(f, n):
        return remote(psend.at[f, n], precv.at[f, n], rs_send.at[0], rs_recv.at[0, n], other_core)

    def to_far(f, n):
        return remote(xsend.at[f, n], xrecv.at[f, n], rs_send.at[1], rs_recv.at[1, n], far)

    def to_near(f, n):
        return remote(ysend.at[f, n], yrecv.at[f, n], rs_send.at[2], rs_recv.at[2, n], near)

    def down_slot(f, dz, ya):
        n = index(dz, ya)
        psend[f, n] = jnp.dot(hid[half:, :], dn[f, n], preferred_element_type=F32).astype(BF16)
        to_sibling(f, n).start()
        keep[n] = jnp.dot(hid[:half, :], dn[f, n], preferred_element_type=F32)

    def add_cores(f, dz, ya):
        n = index(dz, ya)
        to_sibling(f, n).wait_recv()
        xsend[f, n] = (keep[n, 2 * quarter:, :] + precv[f, n, 2 * quarter:, :].astype(F32)).astype(BF16)
        to_far(f, n).start()
        keep[n, :2 * quarter, :] = keep[n, :2 * quarter, :] + precv[f, n, :2 * quarter, :].astype(F32)

    def add_far(f, dz, ya):
        n = index(dz, ya)
        to_far(f, n).wait_recv()
        ysend[f, n] = (keep[n, quarter:2 * quarter, :] + xrecv[f, n, quarter:, :].astype(F32)).astype(BF16)
        to_near(f, n).start()
        keep[n, :quarter, :] = keep[n, :quarter, :] + xrecv[f, n, :quarter, :].astype(F32)

    def add_near(f, dz, ya):
        n = index(dz, ya)
        to_near(f, n).wait_recv()
        cols = ds(((z + dz) * YS + ya) * dcols, dcols, dcols)
        br[:, cols] = keep[n, :quarter, :] + yrecv[f, n].astype(F32)

    groups = [(d, dy) for d in range(ZS) for dy in range(YS)]

    stages = {"C": add_cores, "F": add_far, "N": add_near}

    def reduce(f, order, extra_work):
        for i, name in enumerate(order.split()):
            d, dy = groups[int(name[1])]
            act = stages.get(name[0], down_slot)
            if act is down_slot and d:
                arrive(f, (DOWN,), d, (dy,))
            at_distance(d, lambda dz: act(f, dz, lax.rem(y + dy, YS)))
            if name in extra_work:
                extra_work[name]()

    def first_norms():
        @pl.loop(0, quarter // 32)
        def _(i):
            rows = ds(i * 32, 32, 32)
            first = normalize(
                residual_scale * xb[0, rows, :].astype(F32) + 0.5 * br[rows, :], vecs[0], vecs[1]
            ).astype(BF16)
            xb[1, rows, :] = normalize(
                residual_scale * first.astype(F32) + mix[rows, :].astype(F32), vecs[2], vecs[3]
            ).astype(BF16)

    def out_copy(i):
        rows = ds(core * quarter + i * 32, 32, 32)
        return remote(out_ref.at[rows], out_ref.at[rows], fin_sem.at[0], fin_sem.at[1], other_core)

    def last_norm():
        @pl.loop(0, quarter // 32)
        def _(i):
            rows = ds(i * 32, 32, 32)
            out_ref[ds(core * quarter + i * 32, 32, 32), :] = normalize(
                residual_scale * xb[1, rows, :].astype(F32) + 0.5 * br[rows, :], vecs[4], vecs[5]
            ).astype(BF16)
            out_copy(i).start()

    def pair_sent_wait(f):
        for i in range(3):
            pair_landing(f, i).wait_send()

    def z_sent_wait(f):
        for way, sign in (("up", -1), ("dn", 1)):
            for planes in STEPS:
                @pl.when(z == (planes - 1 if sign < 0 else ZS - planes))
                def _():
                    for piece in range(3):
                        gone = (gum, gux, dn)[piece].at[f, pl.ds(0, planes * (YS if piece == DOWN else 1))]
                        sem = zs_send.at[f, piece, int(way == "up")]
                        remote(gone, gone, sem, sem, other_core).wait_send()

    def reduce_sent_wait(f):
        for i, gone in enumerate((psend.at[f], xsend.at[f], ysend.at[f])):
            remote(gone, gone, rs_send.at[i], rs_send.at[i], other_core).wait_send()

    def load_wait(f, i):
        landed = (gum.at[f, 0, ds(y * ks, ks, ks)], dn.at[f, y], raw.at[f])[i]
        pltpu.make_async_copy(landed, landed, local.at[3 * f + i]).wait()

    outer = jnp.logical_not(inner)

    def outer_middle():
        @pl.when(outer)
        def _():
            pair_wait(1, range(3))

        own_all(1)

    def inner_middle():
        forward(0, (DOWN,), 2)

        @pl.when(inner)
        def _():
            pair_wait(1, range(3))

        own_send(1, GATE_UP, 0, inner)
        own_send(1, GATE_UP, 1, inner)

    pair_start(0, (0, 1))
    load_wait(0, 0)
    own_send(0, (MAIN,), 0)
    load_wait(0, 2)
    pack(0)
    pair_start(0, (2,))
    own_send(0, (EXTRA,), 0)
    token_loads[0].wait()
    gather_start(0)
    pair_start(0, (3, 4))
    load_wait(0, 1)
    own_send(0, (DOWN,), 0)
    load_wait(1, 0)
    load_wait(1, 1)
    load_wait(1, 2)
    pack(1)
    pair_wait(0, (0, 1))
    own_send(0, GATE_UP, 1)
    forward(0, GATE_UP, 1, (0,))
    gather_near(0)
    forward(0, GATE_UP, 1, (1,))
    gather_far(0)
    forward(0, GATE_UP, 2, (0,))
    pair_start(1, range(5))
    pair_wait(0, (2,))
    own_send(0, (DOWN,), 1, outer)
    token_loads[1].wait()
    gather_wait(0)
    gate_up(0, 0, first=True)
    forward(0, GATE_UP, 2, (1,))
    arrive(0, GATE_UP, 1)
    at_distance(1, lambda dz: gate_up(0, dz))
    own_send(0, (DOWN,), 1, inner)
    arrive(0, GATE_UP, 2)
    at_distance(2, lambda dz: gate_up(0, dz))
    outer_middle()
    arrive(0, GATE_UP, 3)
    at_distance(3, lambda dz: gate_up(0, dz))
    activate()
    forward(0, (DOWN,), 1)
    reduce(0, FIRST_ORDER, {"D3": inner_middle, "F3": lambda: forward(1, GATE_UP, 1)})
    for load in [mixer_load] + vec_loads:
        load.wait()
    first_norms()
    gather_sent_wait(0)
    reduce_sent_wait(0)
    gather_start(1)
    gather_near(1)
    forward(1, GATE_UP, 2)
    own_send(1, (DOWN,), 0, inner)
    own_send(1, (DOWN,), 1, inner)
    gather_far(1)
    gather_wait(1)
    gate_up(1, 0, first=True)
    forward(1, (DOWN,), 1)
    arrive(1, GATE_UP, 1)
    at_distance(1, lambda dz: gate_up(1, dz))
    forward(1, (DOWN,), 2)
    arrive(1, GATE_UP, 2)
    at_distance(2, lambda dz: gate_up(1, dz))
    pair_sent_wait(0)
    pair_sent_wait(1)
    z_sent_wait(0)
    arrive(1, GATE_UP, 3)
    at_distance(3, lambda dz: gate_up(1, dz))
    activate()
    reduce(1, LAST_ORDER, {"F7": lambda: z_sent_wait(1)})
    gather_sent_wait(1)
    reduce_sent_wait(1)
    last_norm()
    gone, landed = out_ref.at[mine], out_ref.at[sib]
    remote(gone, landed, fin_sem.at[0], fin_sem.at[1], other_core).wait()


def per_device(
    tokens, mixer_out, gate_first, up_first, down_first, gate_second, up_second, down_second,
    gain_first, bias_first, gain_middle, bias_middle, gain_last, bias_last,
):
    rows, width = tokens.shape
    ks, hidden = gate_first.shape
    dcols = down_first.shape[1]
    quarter = rows // 2
    main, extra = split(hidden)
    wide = -(-2 * extra // 128) * 128
    slots = ZS * YS

    any_spec, vmem = pl.BlockSpec(memory_space=pl.ANY), pl.BlockSpec(memory_space=pltpu.VMEM)
    vec = lambda v: v.reshape(1, width)
    dma = pltpu.SemaphoreType.DMA
    return pl.pallas_call(
        kernel,
        out_shape=pltpu.VMEM((rows, width), BF16),
        in_specs=[any_spec] * 14,
        out_specs=pl.BlockSpec(memory_space=pltpu.VMEM),
        scratch_shapes=[
            pltpu.VMEM((6, 1, width), F32),
            pltpu.VMEM((2, ZS, YS * ks, 2 * main), BF16),
            pltpu.VMEM((2, ZS, YS * ks // 2, 4 * extra), BF16),
            pltpu.VMEM((2, 2, ks, 4 * extra), BF16),
            pltpu.VMEM((2, ks // 2, 4 * extra), BF16),
            pltpu.VMEM((2, slots, main + extra, dcols), BF16),
            pltpu.VMEM((2, 8 * quarter, width), BF16),
            pltpu.VMEM((8 * quarter, 2 * main), F32),
            pltpu.VMEM((8 * quarter, wide), F32),
            pltpu.VMEM((8 * quarter, wide), F32),
            pltpu.VMEM((8 * quarter, main + extra), BF16),
            pltpu.VMEM((slots, 4 * quarter, dcols), F32),
            pltpu.VMEM((2, slots, 4 * quarter, dcols), BF16),
            pltpu.VMEM((2, slots, 4 * quarter, dcols), BF16),
            pltpu.VMEM((2, slots, 2 * quarter, dcols), BF16),
            pltpu.VMEM((2, slots, 2 * quarter, dcols), BF16),
            pltpu.VMEM((2, slots, quarter, dcols), BF16),
            pltpu.VMEM((2, slots, quarter, dcols), BF16),
            pltpu.VMEM((quarter, width), F32),
            pltpu.VMEM((quarter, width), BF16),
            dma((2, 3, 2)), dma((2, 2, ZS - 1, YS)),
            dma((2, 3)), dma((2, 3)),
            dma((1,)), dma((7,)),
            dma((3,)), dma((3, slots)),
            dma((2,)),
            dma((15,)),
        ],
        compiler_params=pltpu.CompilerParams(
            collective_id=0, has_side_effects=True, vmem_limit_bytes=60 * 1024 * 1024
        ),
    )(
        tokens, mixer_out,
        gate_first, up_first, down_first, gate_second, up_second, down_second,
        vec(gain_first), vec(bias_first), vec(gain_middle), vec(bias_middle), vec(gain_last), vec(bias_last),
    )


def split(hidden):
    main = hidden // 4 // 128 * 128
    return main, hidden // 4 - main


def on_mesh(mesh, rows, width, hidden):
    sizes = dict(mesh.shape)
    if (sizes["rep"], sizes["fs"], sizes["tp"]) != (2, ZS * YS, 2):
        return False
    rows, ks, hidden = rows // (2 * ZS * YS), width // (ZS * YS), hidden // 2
    main, extra = split(hidden)
    span = ks * 2 * (main + extra)
    fits = rows % 32 == 0 and ks % 256 == 0 and hidden % 128 == 0 and span % (8 * width) == 0
    return fits and main > 0 and extra > 0 and extra % 32 == 0


def solution(mesh):
    def run(tokens, mixer_out, gate_first, *rest):
        fits = on_mesh(mesh, tokens.shape[0], tokens.shape[1], gate_first.shape[1])
        return jax.shard_map(
            per_device if fits else per_device_general,
            mesh=mesh,
            in_specs=(
                P(("rep", "fs"), None), P(("rep", "fs"), None),
                P("fs", "tp"), P("fs", "tp"), P("tp", "fs"),
                P("fs", "tp"), P("fs", "tp"), P("tp", "fs"),
                P(), P(), P(), P(), P(), P(),
            ),
            out_specs=P(("rep", "fs"), None),
            check_vma=False,
        )(tokens, mixer_out, gate_first, *rest)

    return run
```
